512 devices in a mesh: ep: 32 (over z, core), tp: 16 (over y, x).
Axes of the slice: x: 4, y: 4, z: 16, core: 2. Of those that a mesh axis runs over, the one named last changes fastest.
Arguments:
- query_rows: bfloat16 [12288, 2048], P('ep', 'tp'), may hold values from -6 to 6
- key_rows: bfloat16 [12288, 2048], P('ep', 'tp'), may hold values from -6 to 6
- value_rows: bfloat16 [12288, 2048], P('ep', 'tp'), may hold values from -6 to 6
- second_scale: float32 [16], P('tp'), may hold values from 0.3 to 0.8
- head_gain: float32 [128], replicated, may hold values from 0.1 to 1.9
- out_weight: bfloat16 [2048, 4096], P(None, 'tp'), may hold values from -0.125 to 0.125
- routed_rows: bfloat16 [4096, 4096], P('ep', 'tp'), may hold values from -6 to 6
- norm_gain: float32 [4096], replicated, may hold values from 0.1 to 1.9
- route_ids: int32 [4096, 2], P('ep'), may hold values from 0 to 31, all different within a row; in each aligned block of 128 rows (0 to 127, 128 to 255, ...) at most 16 rows name the same one
- route_weight: float32 [4096, 2], P('ep'), may hold values from 0.1 to 0.9
- expert_gate: bfloat16 [32, 4096, 2048], P('ep', None, 'tp'), may hold values from -0.09375 to 0.09375
- expert_up: bfloat16 [32, 4096, 2048], P('ep', None, 'tp'), may hold values from -0.09375 to 0.09375
- expert_down: bfloat16 [32, 2048, 4096], P('ep', None, 'tp'), may hold values from -0.125 to 0.125
Outputs:
- mixer_out: bfloat16 [12288, 4096], P('ep', 'tp')
- expert_mix: bfloat16 [4096, 4096], P('ep', 'tp')
The draws below stay inside these ranges and needn't reach their ends.
Inputs may be any that keep to these rules, and one draw needn't show every extreme that they name: `route_ids`: among the 128 tokens of one index of ep, no expert is named by more than 16 of them, a bound that some block reaches.
All inputs are finite; a program needn't handle non-finite values.
Results may differ from the reference program's by a relative error of at most 0.0085.
Values may be sent and summed in bfloat16 or wider, within the bound.
A program may use at most 64 MiB of HBM per device.

```python
import math
import jax
import jax.numpy as jnp
import numpy as np
from jax import lax

D = 4096
HEADS = 16
HD = 64
VD = 128
FF = 2048
TOP = 2
TOK_A = 384
TOK_B = 128
TOKENS_A = 12288
TOKENS_B = 4096
EXPERTS = 32
CAP = 16
N_EP = 32


def draw_query_rows(key, part):
    length_all = TOK_A * N_EP
    drawn_rows = jnp.clip(1.3 * jax.random.normal(jax.random.fold_in(key, 3), (length_all, HEADS * 2 * HD), jnp.float32), -6.0, 6.0)
    return drawn_rows.astype(jnp.bfloat16)


def draw_key_rows(key, part):
    length_all = TOK_A * N_EP
    drawn_rows = jnp.clip(1.3 * jax.random.normal(jax.random.fold_in(key, 5), (length_all, HEADS * 2 * HD), jnp.float32), -6.0, 6.0)
    return drawn_rows.astype(jnp.bfloat16)


def level_of(rng, shape, split, smallest, largest):
    factor_of = 1.0
    for axis_at, parts in split:
        draws = jax.random.uniform(jax.random.fold_in(jax.random.fold_in(rng, 6), axis_at), (parts,), jnp.float32, smallest / len(split), largest / len(split))
        factor_of = factor_of * jnp.repeat(jnp.exp(draws), shape[axis_at] // parts).reshape((-1,) + (1,) * (len(shape) - 1 - axis_at))
    return factor_of


def deal_out(stream_key, own, number, rows, number_of, top, bound, slope):
    order = jax.random.permutation(stream_key, number_of)
    crowded, ordinary = load_shares(number_of, rows * top, bound, slope, True), load_shares(number_of, rows * top, bound, slope, False)
    places = jnp.arange(number_of)

    def named(sizes, offset_by):
        used = int((sizes > 0).sum())
        fixed = max(1, used // 4)
        passed = fixed + (places - fixed + offset_by * (used - fixed)) % max(1, number_of - fixed)
        return jnp.zeros((number_of,), jnp.int32).at[order[jnp.where(places < fixed, places, passed)]].set(jnp.asarray(sizes, jnp.int32))

    sizes = jnp.where(number % 4 == 0, named(crowded, number // 4), named(ordinary, number - number // 4 - 1))
    mixed = jax.random.permutation(jax.random.fold_in(own, 3), number_of)
    giver, sink = mixed[0:number_of // 2 * 2:2], mixed[1:number_of // 2 * 2:2]
    margin = jnp.minimum(sizes[giver] - 1, bound - sizes[sink]) // 2
    margin = jnp.where((giver == order[0]) | (sink == order[0]) | (sizes[sink] == 0), 0, jnp.maximum(margin, 0))
    passed = jax.random.randint(jax.random.fold_in(own, 4), (number_of // 2,), 0, 1 << 20) % (margin + 1)
    sizes = sizes.at[giver].add(-passed).at[sink].add(passed)
    labels = jnp.searchsorted(jnp.cumsum(sizes), jnp.arange(rows * top), side="right").astype(jnp.int32)
    table = labels.reshape(top, rows).T
    table = table[jax.random.permutation(jax.random.fold_in(own, 1), rows)]
    offset_by = jax.random.randint(jax.random.fold_in(own, 2), (rows, 1), 0, top)
    return jnp.take_along_axis(table, (jnp.arange(top)[None, :] + offset_by) % top, axis=1)


def load_shares(amount, total, limit, slope, full):
    loads = [(1 << 20) // math.isqrt(rank ** slope) + 1 for rank in range(1, amount + 1)]
    largest = limit if full else min(limit, max(-(-total // amount), total * loads[0] // sum(loads)))
    least = 1 if total - largest >= amount - 1 else 0
    given, spare = [largest] + [least] * (amount - 1), total - largest - least * (amount - 1)
    while spare > 0:
        free = [i for i in range(1, amount) if given[i] < largest] or [i for i in range(1, amount) if given[i] < limit]
        pool, remaining = sum([loads[i] for i in free]), spare
        for i in free:
            more = min(limit - given[i], max(1, remaining * loads[i] // pool), spare)
            given[i] = given[i] + more
            spare = spare - more
    return np.array(given)


def normal_values(key, dims, spread, reach, pieces=(), held_as=jnp.bfloat16):
    level = level_of(key, dims, pieces, -0.22, 0.18) if pieces else 1.0
    values = jax.random.normal(key, dims, jnp.float32) * spread * level
    return jnp.minimum(jnp.maximum(values, -reach), reach).astype(held_as)


def setup_inputs(seed: int = 0) -> dict:
    keys = jax.random.split(jax.random.key(seed), 14)
    query_rows = draw_query_rows(jax.random.fold_in(keys[13], 71), 0)
    key_rows = draw_key_rows(jax.random.fold_in(keys[13], 71), 0)
    value_rows = normal_values(keys[2], (TOKENS_A, HEADS * VD), 1.0, 6.0, ((0, 32), (1, 16)))
    second_scale = jnp.clip(0.3 + 0.5 * jax.random.uniform(keys[3], (HEADS,), jnp.float32) ** level_of(keys[3], (HEADS,), ((0, 16),), -0.2, 0.2), 0.3, 0.8)
    head_gain = jnp.clip(1.0 + 0.18 * jax.random.normal(keys[4], (VD,), jnp.float32), 0.1, 1.9)
    out_weight = normal_values(keys[5], (HEADS * VD, D), (HEADS * VD) ** -0.5, 0.125, ((1, 16),))
    routed_rows = normal_values(keys[6], (TOKENS_B, D), 1.0, 6.0, ((0, 32), (1, 16)))
    norm_gain = jnp.clip(1.0 + 0.18 * jax.random.normal(keys[7], (D,), jnp.float32), 0.1, 1.9)
    route_ids_keys = jax.random.split(jax.random.fold_in(keys[8], 1), TOKENS_B // TOK_B)
    route_ids_turns = jax.random.permutation(jax.random.fold_in(keys[8], 3), TOKENS_B // TOK_B)
    route_ids = jax.vmap(lambda own, number: deal_out(jax.random.fold_in(keys[8], 2), own, number, TOK_B, EXPERTS, TOP, CAP, 1))(route_ids_keys, route_ids_turns).reshape((TOKENS_B, TOP))
    route_weight = jnp.clip(0.1 + 0.79999997 * jax.random.uniform(keys[9], (TOKENS_B, TOP), jnp.float32) ** level_of(keys[9], (TOKENS_B, TOP), ((0, 32),), -0.2, 0.2), 0.1, 0.9)
    expert_gate = normal_values(keys[10], (EXPERTS, D, FF), D ** -0.5, 0.09375, ((0, 32), (2, 16)))
    expert_up = normal_values(keys[11], (EXPERTS, D, FF), D ** -0.5, 0.09375, ((0, 32), (2, 16)))
    expert_down = normal_values(keys[12], (EXPERTS, FF, D), FF ** -0.5, 0.125, ((0, 32), (2, 16)))
    return {"query_rows": query_rows, "key_rows": key_rows, "value_rows": value_rows, "second_scale": second_scale, "head_gain": head_gain, "out_weight": out_weight, "routed_rows": routed_rows, "norm_gain": norm_gain, "route_ids": route_ids, "route_weight": route_weight, "expert_gate": expert_gate, "expert_up": expert_up, "expert_down": expert_down}


eps = 1e-06
head_factor = 0.8
neg_big = -1e+30

def rms_rows(rows_in, gain):
    floats = rows_in.astype(jnp.float32)
    factor = lax.rsqrt(lax.optimization_barrier(jnp.mean(floats * floats, axis=-1, keepdims=True)) + eps)
    return (floats * factor * gain).astype(jnp.bfloat16)

def reference(query_rows, key_rows, value_rows, second_scale, head_gain, out_weight, routed_rows, norm_gain, route_ids, route_weight, expert_gate, expert_up, expert_down):
    length_all = query_rows.shape[0]
    block_rows = min(512, length_all)
    positions = jnp.arange(length_all, dtype=jnp.int32)
    query_heads = jnp.transpose(query_rows.reshape(length_all, HEADS, 2, HD), (1, 0, 2, 3))
    key_heads = jnp.transpose(key_rows.reshape(length_all, HEADS, 2, HD), (1, 0, 2, 3))
    value_heads = jnp.transpose(value_rows.reshape(length_all, HEADS, VD), (1, 0, 2))

    def one_head(operands):
        query_h, key_h, value_h, scale_h = operands
        key_float = key_h.astype(jnp.float32)
        value_float = value_h.astype(jnp.float32)

        def one_block(block_num):
            row_first = block_num * block_rows
            query_block = lax.dynamic_slice_in_dim(query_h, row_first, block_rows, 0).astype(jnp.float32)
            scores = jnp.einsum('icd,jcd->cij', query_block, key_float) * HD ** (-0.5)
            allowed = ((row_first + jnp.arange(block_rows, dtype=jnp.int32))[:, None] >= positions[None, :])[None]
            scores = jnp.where(allowed, scores, neg_big)
            row_max = lax.optimization_barrier(jnp.max(scores, axis=-1, keepdims=True))
            exp_scores = jnp.where(allowed, jnp.exp(scores - row_max), 0.0)
            denoms = lax.optimization_barrier(jnp.sum(exp_scores, axis=-1))
            rounded = lax.optimization_barrier(exp_scores.astype(jnp.bfloat16)).astype(jnp.float32)
            maps_both = jnp.einsum('cij,je->cie', rounded, value_float) / denoms[..., None]
            mixed_maps = maps_both[0] - scale_h * maps_both[1]
            mean_sq = lax.optimization_barrier(jnp.mean(mixed_maps * mixed_maps, axis=-1, keepdims=True))
            return (mixed_maps * lax.rsqrt(mean_sq + eps) * head_gain * head_factor).astype(jnp.bfloat16)
        block_outs = lax.map(one_block, jnp.arange(length_all // block_rows, dtype=jnp.int32))
        return block_outs.reshape(length_all, VD)
    head_outs = lax.map(one_head, (query_heads, key_heads, value_heads, second_scale))
    head_cat = jnp.transpose(head_outs, (1, 0, 2)).reshape(length_all, HEADS * VD)
    mixer_out = jnp.dot(head_cat, out_weight, preferred_element_type=jnp.float32).astype(jnp.bfloat16)
    normed = rms_rows(routed_rows, norm_gain)
    flat_expert = route_ids.reshape(-1).astype(jnp.int32)
    count_all = flat_expert.shape[0]
    chosen = (flat_expert[:, None] == jnp.arange(EXPERTS, dtype=jnp.int32)[None, :]).astype(jnp.int32)
    ranks = lax.optimization_barrier(jnp.sum((jnp.cumsum(chosen, axis=0) - 1) * chosen, axis=1)).astype(jnp.int32)
    token_of = jnp.arange(count_all, dtype=jnp.int32) // TOP
    table = jnp.full((EXPERTS, N_EP * CAP), TOKENS_B, jnp.int32).at[flat_expert, ranks].set(token_of)
    padded = jnp.concatenate([normed, jnp.zeros((1, D), jnp.bfloat16)], axis=0)

    def one_expert(operands):
        table_row, gate_w, up_w, down_w = operands
        gathered = padded[table_row]
        gate_val = jnp.dot(gathered, gate_w, preferred_element_type=jnp.float32)
        up_val = jnp.dot(gathered, up_w, preferred_element_type=jnp.float32)
        hidden = (jax.nn.silu(gate_val) * up_val).astype(jnp.bfloat16)
        return jnp.dot(hidden, down_w, preferred_element_type=jnp.float32).astype(jnp.bfloat16)
    expert_outs = lax.map(one_expert, (table, expert_gate, expert_up, expert_down))
    picked = expert_outs[flat_expert, ranks].astype(jnp.float32).reshape(TOKENS_B, TOP, D)
    expert_mix = lax.optimization_barrier(jnp.sum(picked * route_weight[:, :, None], axis=1)).astype(jnp.bfloat16)
    return (mixer_out, expert_mix)
```

```python
import functools
import math

import jax
import jax.numpy as jnp
from jax import lax
from jax.experimental import pallas as pl
from jax.experimental.pallas import tpu as pltpu
from jax.sharding import PartitionSpec as P

MESH = pl.DeviceIdType.MESH
F32 = jnp.float32
BF16 = jnp.bfloat16
EPS = 1e-06
HEAD_FACTOR = 0.8
NEG = -1e30
PLANE = {16: (4, 4), 1: (1, 1)}


def dot(a, b):
    return lax.dot_general(a, b, (((1,), (0,)), ((), ())), preferred_element_type=F32)


def kernel(
    nz,
    ny,
    nx,
    cap,
    q_ref,
    k_ref,
    v_ref,
    scale_ref,
    hgain_ref,
    wout_hbm,
    x_ref,
    ngain_ref,
    ids_ref,
    rw_ref,
    gate_hbm,
    up_hbm,
    down_hbm,
    mixer_ref,
    mix_ref,
    kbuf,
    vbuf,
    qq,
    m_ref,
    acc,
    ssbuf,
    disp,
    xbuf,
    gu,
    hbuf,
    obuf,
    rbuf,
    hobuf,
    picks,
    wgu,
    wdown,
    wout,
    w_sem,
    own_send,
    own_recv,
    ring_send,
    ring_recv,
    pass_send,
    pass_recv,
    ss_send,
    ss_recv,
    a2a_send,
    a2a_recv,
    xy_send,
    xy_recv,
):
    n_ep, n_tp = 2 * nz, ny * nx
    ta, hd2 = q_ref.shape
    vd = v_ref.shape[1]
    tb, dcol = x_ref.shape
    slots = n_ep * cap
    ff = gate_hbm.shape[1]
    ocol = wdown.shape[1]
    steps = nz // 2

    ep = lax.axis_index("ep")
    tp = lax.axis_index("tp")
    z, c = lax.div(ep, 2), lax.rem(ep, 2)
    y, x = lax.div(tp, nx), lax.rem(tp, nx)

    def at_ep(zz, cc):
        return {"ep": 2 * zz + cc}

    def remote(src, dst, ssem, rsem, dev):
        return pltpu.make_async_remote_copy(
            src_ref=src, dst_ref=dst, send_sem=ssem, recv_sem=rsem, device_id=dev, device_id_type=MESH
        )

    barrier = pltpu.get_barrier_semaphore()

    def greet_ep(i, carry):
        pl.semaphore_signal(barrier, inc=1, device_id={"ep": lax.rem(ep + i, n_ep)}, device_id_type=MESH)
        return carry

    def greet_tp(i, carry):
        pl.semaphore_signal(barrier, inc=1, device_id={"tp": lax.rem(tp + i, n_tp)}, device_id_type=MESH)
        return carry

    lax.fori_loop(1, n_ep, greet_ep, 0)
    if n_tp > 1:
        lax.fori_loop(1, n_tp, greet_tp, 0)

    w_copies = [
        pltpu.make_async_copy(gate_hbm, wgu.at[:, pl.ds(0, ff)], w_sem.at[0]),
        pltpu.make_async_copy(up_hbm, wgu.at[:, pl.ds(ff, ff)], w_sem.at[1]),
        pltpu.make_async_copy(down_hbm, wdown, w_sem.at[2]),
        pltpu.make_async_copy(wout_hbm, wout, w_sem.at[3]),
    ]
    for copy in w_copies:
        copy.start()

    v_t = v_ref[...].astype(F32).T.astype(BF16)

    @pl.when(c == 0)
    def _():
        vbuf[z, 0:vd, 0:ta] = v_t

    @pl.when(c == 1)
    def _():
        vbuf[z, 0:vd, ta : 2 * ta] = v_t

    kbuf[ep] = k_ref[...]
    x_own = x_ref[...].astype(F32)
    squares = jnp.sum((x_own * x_own).T, axis=0, keepdims=True)
    ssbuf[tp] = jnp.broadcast_to(squares, (8, tb))

    def ones_rows(i, carry):
        vbuf[i, vd : vd + 16, :] = jnp.ones((16, 2 * ta), BF16)
        return carry

    lax.fori_loop(0, nz, ones_rows, 0)

    half = hd2 // 2
    q_t = (q_ref[...].astype(F32) * (math.log2(math.e) * half**-0.5)).T
    q_hi = q_t.astype(BF16)
    q_lo = (q_t - q_hi.astype(F32)).astype(BF16)
    none = jnp.zeros((half, ta), BF16)
    for i, part in enumerate((q_hi, q_lo)):
        qq[2 * half * i : 2 * half * i + half, 0:ta] = part[0:half]
        qq[2 * half * i : 2 * half * i + half, ta : 2 * ta] = none
        qq[2 * half * i + half : 2 * half * (i + 1), 0:ta] = none
        qq[2 * half * i + half : 2 * half * (i + 1), ta : 2 * ta] = part[half:]
    m_ref[...] = jnp.full(m_ref.shape, NEG, F32)
    acc[...] = jnp.zeros(acc.shape, F32)

    ids = ids_ref[...]
    lane = lax.broadcasted_iota(jnp.int32, (tb, 128), 1)
    first = jnp.where(ids[:, 0:1] == lane, 1.0, 0.0).astype(F32)
    second = jnp.where(ids[:, 1:2] == lane, 1.0, 0.0).astype(F32)
    lower = jnp.where(
        lax.broadcasted_iota(jnp.int32, (tb, tb), 0) > lax.broadcasted_iota(jnp.int32, (tb, tb), 1), 1.0, 0.0
    ).astype(BF16)
    before_0 = dot(lower, first.astype(BF16))
    before_1 = dot(lower, second.astype(BF16)) + jnp.sum(first, axis=0, keepdims=True)
    rank_0 = jnp.sum(first * before_0, axis=1, keepdims=True)
    rank_1 = jnp.sum(second * before_1, axis=1, keepdims=True)
    slot_0 = ids[:, 0:1].astype(F32) * cap + rank_0
    slot_1 = ids[:, 1:2].astype(F32) * cap + rank_1
    slot_lane = lax.broadcasted_iota(jnp.int32, (tb, slots), 1).astype(F32)
    pick_0 = jnp.where(slot_0 == slot_lane, 1.0, 0.0).astype(F32)
    pick_1 = jnp.where(slot_1 == slot_lane, 1.0, 0.0).astype(F32)
    picks[0] = pick_0.astype(BF16)
    picks[1] = pick_1.astype(BF16)
    spread = (pick_0 + pick_1).T.astype(BF16)

    pl.semaphore_wait(barrier, (n_ep - 1) + (n_tp - 1))

    def k_at(zz, cc):
        return kbuf.at[2 * zz + cc]

    def v_at(zz, cc):
        return vbuf.at[zz, pl.ds(0, vd), pl.ds(pl.multiple_of(cc * ta, 128), ta)]

    part_at = (k_at, v_at)

    def wrap(zz):
        return lax.rem(zz + nz, nz)

    def hop(direction, s, kv, owner):
        ref = part_at[kv](owner, c)
        to = wrap(z + 1) if direction == 0 else wrap(z - 1)
        return remote(
            ref, ref, ring_send.at[direction, s, kv], ring_recv.at[direction, s, kv], at_ep(to, c)
        )

    def handover(direction, s, kv, owner):
        ref = part_at[kv](owner, c)
        return remote(
            ref, ref, pass_send.at[direction, s, kv], pass_recv.at[direction, s, kv], at_ep(z, 1 - c)
        )

    def handed(direction, s, kv, owner):
        ref = part_at[kv](owner, 1 - c)
        return remote(
            ref, ref, pass_send.at[direction, s, kv], pass_recv.at[direction, s, kv], at_ep(z, 1 - c)
        )

    def owner_of(direction, s):
        return wrap(z - s) if direction == 0 else wrap(z + s)

    last = (steps, nz - 1 - steps)
    for kv in range(2):
        for direction in range(2):
            if last[direction] >= 1:
                hop(direction, 1, kv, z).start()
        handover(0, 0, kv, z).start()

    def ring_tick(s):
        for direction in range(2):

            @pl.when(s <= last[direction])
            def _(direction=direction):
                for kv in range(2):
                    owner = owner_of(direction, s)
                    hop(direction, s, kv, owner).wait_recv()

                    @pl.when(s < last[direction])
                    def _(direction=direction, kv=kv, owner=owner):
                        hop(direction, s + 1, kv, owner).start()

                    handover(direction, s, kv, owner).start()

    n_tile = 256 if (2 * ta) % 256 == 0 else 2 * ta

    def attend(owner, masked):
        keys = kbuf[pl.ds(2 * owner, 2)].reshape(2 * ta, hd2)
        keys = jnp.concatenate([keys, keys], axis=1)
        values = vbuf[owner]
        for n in range(2 * ta // n_tile):
            cols = slice(n * n_tile, (n + 1) * n_tile)
            s = dot(keys, qq[:, cols])
            if masked:
                row = lax.broadcasted_iota(jnp.int32, s.shape, 0)
                col = lax.broadcasted_iota(jnp.int32, s.shape, 1) + n * n_tile
                col = jnp.where(col >= ta, col - ta, col) + c * ta
                s = jnp.where(row <= col, s, NEG)
            old = m_ref[:, cols]
            new = jnp.maximum(old, jnp.max(s, axis=0, keepdims=True))
            weights = jnp.exp2(s - new).astype(BF16)
            shrink = jnp.exp2(old - new)
            m_ref[:, cols] = new
            acc[:, cols] = acc[:, cols] * shrink + dot(values, weights)

    def ss_copy(i):
        peer = lax.rem(tp + i, n_tp)
        return remote(ssbuf.at[tp], ssbuf.at[tp], ss_send.at[i], ss_recv.at[i], {"tp": peer})

    def ss_from(i):
        ref = ssbuf.at[lax.rem(tp - i + n_tp, n_tp)]
        return remote(ref, ref, ss_send.at[i], ss_recv.at[i], {"tp": lax.rem(tp + i, n_tp)})

    def loop(lo, hi, f):
        if hi > lo:
            lax.fori_loop(lo, hi, lambda i, carry: (f(i), carry)[1], 0)

    loop(1, n_tp, lambda i: ss_copy(i).start())

    for kv in range(2):
        handed(0, 0, kv, z).wait_recv()
    attend(z, True)

    loop(1, n_tp, lambda i: ss_from(i).wait_recv())
    total = ssbuf[0, 0:1, :]
    for i in range(1, n_tp):
        total = total + ssbuf[i, 0:1, :]
    factor = lax.rsqrt(total / (n_tp * dcol) + EPS)
    factor = jnp.broadcast_to(factor, (128, tb)).T
    factor = jnp.concatenate([factor] * (dcol // 128), axis=1)
    gain = ngain_ref[:, pl.ds(pl.multiple_of(tp * dcol, 128), dcol)]
    normed = (x_ref[...].astype(F32) * factor * gain).astype(BF16)
    disp[...] = dot(spread, normed).astype(BF16)

    def dispatch_copy(peer):
        return remote(
            disp.at[pl.ds(pl.multiple_of(peer * cap, cap), cap)],
            xbuf.at[tp, pl.ds(pl.multiple_of(ep * cap, cap), cap)],
            a2a_send.at[0, peer],
            a2a_recv.at[0, ep],
            {"ep": peer},
        )

    def dispatched(source):
        return remote(
            disp.at[pl.ds(pl.multiple_of(source * cap, cap), cap)],
            xbuf.at[tp, pl.ds(pl.multiple_of(source * cap, cap), cap)],
            a2a_send.at[0, source],
            a2a_recv.at[0, source],
            {"ep": source},
        )

    def return_copy(peer):
        return remote(
            obuf.at[pl.ds(pl.multiple_of(peer * cap, cap), cap)],
            rbuf.at[pl.ds(pl.multiple_of(ep * cap, cap), cap)],
            a2a_send.at[1, peer],
            a2a_recv.at[1, ep],
            {"ep": peer},
        )

    def returned(source):
        return remote(
            obuf.at[pl.ds(pl.multiple_of(source * cap, cap), cap)],
            rbuf.at[pl.ds(pl.multiple_of(source * cap, cap), cap)],
            a2a_send.at[1, source],
            a2a_recv.at[1, source],
            {"ep": source},
        )

    def others(f):
        def each(i):
            chip, core = lax.div(i, 2), lax.rem(i, 2)
            d = steps - lax.div(chip + 1, 2)
            zz = lax.rem(jnp.where(lax.rem(chip, 2) == 1, z + d, z - d + nz), nz)
            f(2 * zz + core)

        if nz > 1:
            loop(0, 2 * (nz - 1), each)
        f(2 * z + 1 - c)

    others(lambda peer: dispatch_copy(peer).start())
    mine = pl.ds(pl.multiple_of(ep * cap, cap), cap)
    xbuf[tp, mine, :] = disp[mine, :]

    def plane_gather(number, rows, block):
        quarter = rows // 2

        def half_stages(h):
            size_p, size_s = (nx, ny) if h == 0 else (ny, nx)
            p, s = (x, y) if h == 0 else (y, x)

            def index(ss, pp):
                ss, pp = lax.rem(ss + 4, 4), lax.rem(pp + 4, 4)
                return ss * nx + pp if h == 0 else pp * nx + ss

            rel = (0, -1, 1, 2)
            whole, low, high = (0, rows), (0, quarter), (quarter, quarter)

            def msg(name, ds, dp, part):
                sem = {"pr": 0, "pl": 1, "fr": 2, "fl": 3}.get(name)
                if sem is None:
                    sem = 4 + 4 * ("su", "sd", "gu", "gd").index(name[:2]) + int(name[2])
                ts, tp_ = {
                    "pr": (0, 1), "pl": (0, -1), "fr": (0, 1), "fl": (0, -1),
                    "su": (1, 0), "sd": (-1, 0), "gu": (1, 0), "gd": (-1, 0),
                }[name if sem < 4 else name[:2]]
                ref = block(h, index(s + ds, p + dp), *part)
                return remote(
                    ref, ref, xy_send.at[number, h, sem], xy_recv.at[number, h, sem], {"tp": index(s + ts, p + tp_)}
                )

            sent = []

            def send(name, ds, dp, part):
                msg(name, ds, dp, part).start()
                sent.append(lambda: msg(name, ds, dp, part).wait_send())

            def out(j):
                send(f"su{j}", 0, rel[j], whole)
                send(f"sd{j}", 0, rel[j], whole)

            def forward(j):
                msg(f"su{j}", -1, rel[j], whole).wait_recv()
                send(f"gu{j}", -1, rel[j], low)
                msg(f"sd{j}", 1, rel[j], whole).wait_recv()
                send(f"gd{j}", 1, rel[j], high)

            def ended(j):
                msg(f"gu{j}", -2, rel[j], low).wait_recv()
                msg(f"gd{j}", 2, rel[j], high).wait_recv()

            def stage0():
                send("pr", 0, 0, whole)
                send("pl", 0, 0, whole)
                out(0)

            def stage1():
                msg("pr", 0, -1, whole).wait_recv()
                send("fr", 0, -1, low)
                out(1)
                msg("pl", 0, 1, whole).wait_recv()
                send("fl", 0, 1, high)
                out(2)

            def stage2():
                msg("fr", 0, -2, low).wait_recv()
                msg("fl", 0, 2, high).wait_recv()
                out(3)
                forward(0)

            def stage3():
                forward(1)
                forward(2)

            def stage4():
                forward(3)
                for j in range(3):
                    ended(j)

            def stage5():
                ended(3)

            return (stage0, stage1, stage2, stage3, stage4, stage5), sent

        if n_tp == 1:
            return [lambda: None] * 6, lambda: None
        (a, sent_a), (b, sent_b) = half_stages(0), half_stages(1)

        def both(i):
            a[i]()
            b[i]()

        def drained():
            for wait in sent_a + sent_b:
                wait()

        return [functools.partial(both, i) for i in range(6)], drained

    rows_x = slots // 2

    def x_block(h, owner, row, count):
        return xbuf.at[owner, pl.ds(h * rows_x + row, count)]

    def h_block(h, owner, row, count):
        return hbuf.at[pl.ds(h * rows_x + row, count), pl.ds(pl.multiple_of(owner * ff, 128), ff)]

    rows_a = ta // 2

    def ho_block(h, owner, row, count):
        return hobuf.at[pl.ds(h * rows_a + row, count), pl.ds(pl.multiple_of(owner * vd, 128), vd)]

    x_stages, x_sent = plane_gather(0, rows_x, x_block)
    h_stages, h_sent = plane_gather(1, rows_x, h_block)
    o_stages, o_sent = plane_gather(2, rows_a, ho_block)

    def arrive():
        def wait(i):
            dispatched(lax.rem(ep + i, n_ep)).wait_recv()

        loop(1, n_ep, wait)
        x_stages[0]()

    def experts():
        w_copies[0].wait()
        w_copies[1].wait()
        gu[...] = jnp.zeros(gu.shape, F32)

        def block(t):
            gu[...] += dot(xbuf[t], wgu[pl.ds(pl.multiple_of(t * dcol, dcol), dcol), :])

        loop(0, n_tp, block)
        gate, up = gu[:, 0:ff], gu[:, ff : 2 * ff]
        hidden = (gate / (1.0 + jnp.exp(-gate)) * up).astype(BF16)
        hbuf[:, pl.ds(pl.multiple_of(tp * ff, 128), ff)] = hidden

    def x_last():
        x_stages[5]()
        experts()
        h_stages[0]()

    def h_later():
        h_stages[3]()
        h_stages[4]()

    stages = [
        arrive,
        x_stages[1],
        x_stages[2],
        x_stages[3],
        x_stages[4],
        x_last,
        h_stages[1],
        h_stages[2],
        h_later,
    ]

    def pairs(s):
        def one(direction):
            owner_z = jnp.where(direction == 0, z - s, z + s - nz)

            @pl.when(jnp.logical_and(owner_z >= 0, s <= jnp.where(direction == 0, last[0], last[1])))
            def _():
                attend(owner_z, False)

        for direction in range(2):

            @pl.when(jnp.logical_and(s >= 1, s <= last[direction]))
            def _(direction=direction):
                for kv in range(2):
                    handed(direction, s, kv, owner_of(direction, s)).wait_recv()

        @pl.when(s >= 1)
        def _():
            loop(0, 2, one)

    def tick(s):
        ring_tick(s)
        for i, stage in enumerate(stages):
            if i + 1 <= steps + 1:
                pl.when(s == i + 1)(stage)
        pairs(s - 1)

    loop(1, steps + 2, tick)
    for stage in stages[steps + 1 :]:
        stage()

    maps = acc[0:vd, :] / acc[vd : vd + 1, :]
    mixed = maps[:, 0:ta] - scale_ref[0] * maps[:, ta : 2 * ta]
    mean_sq = jnp.mean(mixed * mixed, axis=0, keepdims=True)
    head = (mixed * lax.rsqrt(mean_sq + EPS)).T * hgain_ref[...] * HEAD_FACTOR
    hobuf[:, pl.ds(pl.multiple_of(tp * vd, 128), vd)] = head.astype(BF16)
    o_stages[0]()

    h_stages[5]()
    w_copies[2].wait()
    obuf[...] = dot(hbuf[...], wdown[...]).astype(BF16)
    others(lambda peer: return_copy(peer).start())
    rbuf[mine, :] = obuf[mine, :]

    for stage in o_stages[1:]:
        stage()
    w_copies[3].wait()
    mixer_ref[...] = dot(hobuf[...], wout[...]).astype(BF16)

    loop(1, n_ep, lambda i: returned(lax.rem(ep + i, n_ep)).wait_recv())
    back = rbuf[...]
    weight = rw_ref[...]
    mix_ref[...] = (dot(picks[0], back) * weight[:, 0:1] + dot(picks[1], back) * weight[:, 1:2]).astype(BF16)

    for kv in range(2):
        for direction in range(2):
            if last[direction] >= 1:
                hop(direction, 1, kv, z).wait_send()
        handover(0, 0, kv, z).wait_send()

    def drain(s):
        for direction in range(2):

            @pl.when(s <= last[direction])
            def _(direction=direction):
                for kv in range(2):
                    owner = owner_of(direction, s)
                    handover(direction, s, kv, owner).wait_send()

                    @pl.when(s < last[direction])
                    def _(direction=direction, kv=kv, owner=owner):
                        hop(direction, s + 1, kv, owner).wait_send()

    loop(1, steps + 1, drain)
    loop(1, n_tp, lambda i: ss_copy(i).wait_send())
    others(lambda peer: dispatch_copy(peer).wait_send())
    others(lambda peer: return_copy(peer).wait_send())
    x_sent()
    h_sent()
    o_sent()


def per_device(nz, ny, nx, *args):
    q, k, v, scale, hgain, wout, x, ngain, ids, rw, gate, up, down = args
    ta, hd2 = q.shape
    vd = v.shape[1]
    tb, dcol = x.shape
    n_ep, n_tp = 2 * nz, ny * nx
    cap = 2 * tb * ids.shape[1] // n_ep
    slots = n_ep * cap
    d, ff = gate.shape[1:]
    gate, up, down = gate.reshape(d, ff), up.reshape(d, ff), down.reshape(down.shape[1:])
    ocol = down.shape[1]
    steps = nz // 2
    vmem = pl.BlockSpec(memory_space=pltpu.VMEM)
    hbm = pl.BlockSpec(memory_space=pl.ANY)
    dma = pltpu.SemaphoreType.DMA
    return pl.pallas_call(
        functools.partial(kernel, nz, ny, nx, cap),
        out_shape=(
            jax.ShapeDtypeStruct((ta, wout.shape[1]), BF16),
            jax.ShapeDtypeStruct((tb, ocol), BF16),
        ),
        in_specs=[
            vmem, vmem, vmem, pl.BlockSpec(memory_space=pltpu.SMEM), vmem, hbm, vmem, vmem, vmem, vmem, hbm, hbm, hbm,
        ],
        out_specs=(vmem, vmem),
        scratch_shapes=[
            pltpu.VMEM((n_ep, ta, hd2), BF16),
            pltpu.VMEM((nz, vd + 16, 2 * ta), BF16),
            pltpu.VMEM((2 * hd2, 2 * ta), BF16),
            pltpu.VMEM((1, 2 * ta), F32),
            pltpu.VMEM((vd + 16, 2 * ta), F32),
            pltpu.VMEM((n_tp, 8, tb), F32),
            pltpu.VMEM((slots, dcol), BF16),
            pltpu.VMEM((n_tp, slots, dcol), BF16),
            pltpu.VMEM((slots, 2 * ff), F32),
            pltpu.VMEM((slots, n_tp * ff), BF16),
            pltpu.VMEM((slots, ocol), BF16),
            pltpu.VMEM((slots, ocol), BF16),
            pltpu.VMEM((ta, n_tp * vd), BF16),
            pltpu.VMEM((2, tb, slots), BF16),
            pltpu.VMEM((d, 2 * ff), BF16),
            pltpu.VMEM(down.shape, BF16),
            pltpu.VMEM(wout.shape, BF16),
            dma((4,)),
            dma((1,)),
            dma((1,)),
            dma((2, steps + 1, 2)),
            dma((2, steps + 1, 2)),
            dma((2, steps + 1, 2)),
            dma((2, steps + 1, 2)),
            dma((n_tp,)),
            dma((n_tp,)),
            dma((2, n_ep)),
            dma((2, n_ep)),
            dma((3, 2, 20)),
            dma((3, 2, 20)),
        ],
        compiler_params=pltpu.CompilerParams(
            collective_id=0, has_side_effects=True, vmem_limit_bytes=60 * 1024 * 1024
        ),
        name="layer",
    )(q, k, v, scale, hgain.reshape(1, -1), wout, x, ngain.reshape(1, -1), ids, rw, gate, up, down)


def solution(mesh):
    placed = (
        P("ep", "tp"),
        P("ep", "tp"),
        P("ep", "tp"),
        P("tp"),
        P(),
        P(None, "tp"),
        P("ep", "tp"),
        P(),
        P("ep", None),
        P("ep", None),
        P("ep", None, "tp"),
        P("ep", None, "tp"),
        P("ep", None, "tp"),
    )
    ny, nx = PLANE[mesh.shape["tp"]]
    return jax.shard_map(
        functools.partial(per_device, mesh.shape["ep"] // 2, ny, nx),
        mesh=mesh,
        in_specs=placed,
        out_specs=(P("ep", "tp"), P("ep", "tp")),
        check_vma=False,
    )
```

```python
import functools
import math

import jax
import jax.numpy as jnp
from jax import lax
from jax.experimental import pallas as pl
from jax.experimental.pallas import tpu as pltpu
from jax.sharding import PartitionSpec as P

MESH = pl.DeviceIdType.MESH
F32 = jnp.float32
BF16 = jnp.bfloat16
EPS = 1e-06
HEAD_FACTOR = 0.8
NEG = -1e30
PLANE = {16: (4, 4), 1: (1, 1)}
PLAN = (
    [("x", 0, 0), ("x", 1, 0)],
    {
        0: [("x", 0, 1)],
        1: [("x", 0, 30)],
        2: [("x", 1, 1)],
        3: [("x", 1, 30)],
        4: [("x", 0, 2)],
        5: [("x", 0, 31)],
        6: [("x", 0, 32)],
        7: [("x", 1, 2)],
        8: [("x", 1, 31)],
        9: [("x", 1, 32)],
        11: [("x", 0, 33)],
        12: [("sides", 0, 0)],
        14: [("x", 1, 33)],
        15: [("sides", 1, 0)],
        16: [("x", 0, 5), ("x", 1, 5)],
        18: [("h", 0, 1), ("h", 0, 30)],
        19: [("h", 1, 1), ("h", 1, 30)],
        21: [("h", 0, 2), ("h", 0, 31), ("h", 0, 32)],
        22: [("h", 1, 2)],
        23: [("h", 1, 31)],
        24: [("h", 1, 32)],
        25: [("h", 0, 33)],
        26: [("h", 1, 33)],
        28: [("h", 0, 5), ("h", 1, 5)],
    },
)


def dot(a, b):
    return lax.dot_general(a, b, (((1,), (0,)), ((), ())), preferred_element_type=F32)


def kernel(
    nz,
    ny,
    nx,
    cap,
    q_ref,
    k_ref,
    v_ref,
    scale_ref,
    hgain_ref,
    wout_hbm,
    x_ref,
    ngain_ref,
    ids_ref,
    rw_ref,
    gate_hbm,
    up_hbm,
    down_hbm,
    mixer_ref,
    mix_ref,
    kbuf,
    vbuf,
    qq,
    m_ref,
    acc,
    gs,
    ssq,
    disp,
    xbuf,
    gu,
    hbuf,
    obuf,
    rbuf,
    hobuf,
    picks,
    wgu,
    wdown,
    wout,
    w_sem,
    ring_send,
    ring_recv,
    pass_send,
    pass_recv,
    a2a_send,
    a2a_recv,
    xy_send,
    xy_recv,
):
    n_ep, n_tp = 2 * nz, ny * nx
    ta, hd2 = q_ref.shape
    vd = v_ref.shape[1]
    tb, dcol = x_ref.shape
    slots = n_ep * cap
    ff = gate_hbm.shape[1]
    ocol = wdown.shape[1]
    steps = nz // 2

    ep = lax.axis_index("ep")
    tp = lax.axis_index("tp")
    z, c = lax.div(ep, 2), lax.rem(ep, 2)
    y, x = lax.div(tp, nx), lax.rem(tp, nx)

    def at_ep(zz, cc):
        return {"ep": 2 * zz + cc}

    def remote(src, dst, ssem, rsem, dev):
        return pltpu.make_async_remote_copy(
            src_ref=src, dst_ref=dst, send_sem=ssem, recv_sem=rsem, device_id=dev, device_id_type=MESH
        )

    barrier = pltpu.get_barrier_semaphore()

    def greet_ep(i, carry):
        pl.semaphore_signal(barrier, inc=1, device_id={"ep": lax.rem(ep + i, n_ep)}, device_id_type=MESH)
        return carry

    def greet_tp(i, carry):
        pl.semaphore_signal(barrier, inc=1, device_id={"tp": lax.rem(tp + i, n_tp)}, device_id_type=MESH)
        return carry

    lax.fori_loop(1, n_ep, greet_ep, 0)
    if n_tp > 1:
        lax.fori_loop(1, n_tp, greet_tp, 0)

    w_copies = [
        pltpu.make_async_copy(gate_hbm, wgu.at[:, pl.ds(0, ff)], w_sem.at[0]),
        pltpu.make_async_copy(up_hbm, wgu.at[:, pl.ds(ff, ff)], w_sem.at[1]),
        pltpu.make_async_copy(down_hbm, wdown, w_sem.at[2]),
        pltpu.make_async_copy(wout_hbm, wout, w_sem.at[3]),
    ]
    for copy in w_copies:
        copy.start()

    v_t = v_ref[...].astype(F32).T.astype(BF16)

    @pl.when(c == 0)
    def _():
        vbuf[z, 0:vd, 0:ta] = v_t

    @pl.when(c == 1)
    def _():
        vbuf[z, 0:vd, ta : 2 * ta] = v_t

    kbuf[ep] = k_ref[...]

    def ones_rows(i, carry):
        vbuf[i, vd : vd + 16, :] = jnp.ones((16, 2 * ta), BF16)
        return carry

    lax.fori_loop(0, nz, ones_rows, 0)

    half = hd2 // 2
    q_t = (q_ref[...].astype(F32) * (math.log2(math.e) * half**-0.5)).T
    q_hi = q_t.astype(BF16)
    q_lo = (q_t - q_hi.astype(F32)).astype(BF16)
    none = jnp.zeros((half, ta), BF16)
    for i, part in enumerate((q_hi, q_lo)):
        qq[2 * half * i : 2 * half * i + half, 0:ta] = part[0:half]
        qq[2 * half * i : 2 * half * i + half, ta : 2 * ta] = none
        qq[2 * half * i + half : 2 * half * (i + 1), 0:ta] = none
        qq[2 * half * i + half : 2 * half * (i + 1), ta : 2 * ta] = part[half:]
    m_ref[...] = jnp.full(m_ref.shape, NEG, F32)
    acc[...] = jnp.zeros(acc.shape, F32)
    gu[...] = jnp.zeros(gu.shape, F32)
    ssq[...] = jnp.zeros(ssq.shape, F32)
    for i in range(gs.shape[0]):
        gs[i : i + 1, :] = ngain_ref[:, 128 * i : 128 * (i + 1)]

    def column(row):
        return jnp.broadcast_to(row, (128, tb)).T

    ids = [column(ids_ref[i : i + 1, :].astype(F32)) for i in range(2)]
    lane = lax.broadcasted_iota(jnp.int32, (tb, 128), 1).astype(F32)
    first = jnp.where(ids[0] == lane, 1.0, 0.0).astype(F32)
    second = jnp.where(ids[1] == lane, 1.0, 0.0).astype(F32)
    lower = jnp.where(
        lax.broadcasted_iota(jnp.int32, (tb, tb), 0) > lax.broadcasted_iota(jnp.int32, (tb, tb), 1), 1.0, 0.0
    ).astype(BF16)
    before_0 = dot(lower, first.astype(BF16))
    before_1 = dot(lower, second.astype(BF16)) + jnp.sum(first, axis=0, keepdims=True)
    rank_0 = jnp.sum(first * before_0, axis=1, keepdims=True)
    rank_1 = jnp.sum(second * before_1, axis=1, keepdims=True)
    slot_0 = ids[0][:, 0:1] * cap + rank_0
    slot_1 = ids[1][:, 0:1] * cap + rank_1
    slot_lane = lax.broadcasted_iota(jnp.int32, (tb, slots), 1).astype(F32)
    pick_0 = jnp.where(slot_0 == slot_lane, 1.0, 0.0).astype(F32)
    pick_1 = jnp.where(slot_1 == slot_lane, 1.0, 0.0).astype(F32)
    picks[0] = pick_0.astype(BF16)
    picks[1] = pick_1.astype(BF16)
    disp[...] = dot((pick_0 + pick_1).T.astype(BF16), x_ref[...]).astype(BF16)

    with jax.named_scope("barrier"):
        pl.semaphore_wait(barrier, (n_ep - 1) + (n_tp - 1))

    def loop(lo, hi, f):
        if not isinstance(lo, int) or not isinstance(hi, int) or hi > lo:
            lax.fori_loop(lo, hi, lambda i, carry: (f(i), carry)[1], 0)

    def chip_at(k):
        away = steps - lax.div(k + 1, 2)
        return lax.rem(jnp.where(lax.rem(k, 2) == 1, z + away, z - away + nz), nz)

    def mirrored(k):
        swapped = jnp.where(lax.rem(k, 2) == 1, k + 1, k - 1)
        return jnp.where(jnp.logical_or(k == 0, k == nz - 1), k, swapped)

    def rows_of(i):
        return pl.ds(pl.multiple_of(i * cap, cap), cap)

    def dispatch_copy(i):
        k, core = lax.div(i, 2), lax.rem(i, 2)
        peer = 2 * chip_at(k) + core
        there = 2 * mirrored(k) + c
        return remote(disp.at[rows_of(peer)], xbuf.at[tp, rows_of(there)], a2a_send.at[0, i], a2a_recv.at[0, there], {"ep": peer})

    def dispatched(i):
        peer = 2 * chip_at(lax.div(i, 2)) + lax.rem(i, 2)
        return remote(disp.at[rows_of(peer)], xbuf.at[tp, rows_of(i)], a2a_send.at[0, i], a2a_recv.at[0, i], {"ep": peer})

    def return_copy(i):
        peer = 2 * chip_at(lax.div(i, 2)) + lax.rem(i, 2)
        return remote(obuf.at[rows_of(i)], rbuf.at[rows_of(ep)], a2a_send.at[1, i], a2a_recv.at[1, ep], {"ep": peer})

    def returned(peer):
        return remote(obuf.at[rows_of(0)], rbuf.at[rows_of(peer)], a2a_send.at[1, 0], a2a_recv.at[1, peer], {"ep": peer})

    self_place = 2 * (nz - 1) + c

    def others(lo, hi, f):
        def each(i):
            pl.when(i != self_place)(lambda: f(i))

        loop(lo, hi, each)

    others(0, n_ep, lambda i: dispatch_copy(i).start())
    xbuf[tp, rows_of(self_place), :] = disp[rows_of(ep), :]

    def k_at(zz, cc):
        return kbuf.at[2 * zz + cc]

    def v_at(zz, cc):
        return vbuf.at[zz, pl.ds(0, vd), pl.ds(pl.multiple_of(cc * ta, 128), ta)]

    def part(owner, core, e):
        return (k_at, v_at)[e % 2](owner, core if e < 2 else 1 - core)

    last = jnp.where(c == 0, steps, nz - 1 - steps)
    next_chip = jnp.where(c == 0, lax.rem(z + 1, nz), lax.rem(z - 1 + nz, nz))

    def owner_of(core, s):
        return lax.rem(jnp.where(core == 0, z - s + nz, z + s), nz)

    def comes(core, s):
        low = nz - 2 - steps
        up, down = z - s >= 0, z + s - nz >= 0
        brought = jnp.where(core == 0, up & (s <= steps), (owner_of(core, s) <= low) & (s <= low + 1))
        return brought, brought & ((core == 0) | down)

    def goes(s):
        low = nz - 2 - steps
        return jnp.where(
            c == 0,
            (z + 1 < nz) & (z - (s - 1) >= 0) & (s <= steps),
            (owner_of(c, s - 1) <= low) & (s <= low + 1),
        )

    def hop(s, e):
        ref = part(owner_of(c, s - 1), c, e)
        return remote(ref, ref, ring_send.at[s, e], ring_recv.at[s, e], at_ep(next_chip, c))

    def hopped(s, e):
        ref = part(owner_of(c, s), c, e)
        return remote(ref, ref, ring_send.at[s, e], ring_recv.at[s, e], at_ep(next_chip, c))

    def handover(s, e):
        ref = part(owner_of(c, s), c, e)
        return remote(ref, ref, pass_send.at[s, e], pass_recv.at[s, e], at_ep(z, 1 - c))

    def handed(s, e):
        ref = part(owner_of(1 - c, s), 1 - c, e)
        return remote(ref, ref, pass_send.at[s, e], pass_recv.at[s, e], at_ep(z, 1 - c))

    for e in range(2):
        pl.when(goes(1))(lambda e=e: hop(1, e).start())
        handover(0, e).start()

    def ring_event(s, e):
        brought, used = comes(c, s)

        @pl.when(brought)
        def _():
            hopped(s, e).wait_recv()
            pl.when(goes(s + 1))(lambda: hop(s + 1, e).start())
            pl.when(used)(lambda: handover(s, e).start())

    n_tile = 256 if (2 * ta) % 256 == 0 else 2 * ta
    tiles = 2 * ta // n_tile

    def attend(owner, n, masked):
        cols = pl.ds(pl.multiple_of(n * n_tile, n_tile), n_tile)
        keys = kbuf[pl.ds(2 * owner, 2)].reshape(2 * ta, hd2)
        keys = jnp.concatenate([keys, keys], axis=1)
        s = dot(keys, qq[:, cols])
        if masked:
            row = lax.broadcasted_iota(jnp.int32, s.shape, 0)
            col = lax.broadcasted_iota(jnp.int32, s.shape, 1) + n * n_tile
            col = jnp.where(col >= ta, col - ta, col) + c * ta
            s = jnp.where(row <= col, s, NEG)
        old = m_ref[:, cols]
        new = jnp.maximum(old, jnp.max(s, axis=0, keepdims=True))
        weights = jnp.exp2(s - new).astype(BF16)
        shrink = jnp.exp2(old - new)
        m_ref[:, cols] = new
        acc[:, cols] = acc[:, cols] * shrink + dot(vbuf[owner], weights)

    with jax.named_scope("own_wait"):
        for e in range(2):
            handed(0, e).wait_recv()
            pl.when(goes(1))(lambda e=e: hop(1, 2 + e).start())
    with jax.named_scope("own_attend"):
        loop(0, tiles, lambda n: attend(z, n, True))

    with jax.named_scope("gain"):
        w_copies[0].wait()
        w_copies[1].wait()
        gain = gs[...].T
        for i in range(gs.shape[0]):
            rows = slice(128 * i, 128 * (i + 1))
            wgu[rows, :] = (wgu[rows, :].astype(F32) * gain[:, i : i + 1]).astype(BF16)

    def plane_gather(number, rows, block):
        quarter = rows // 2

        def half_stages(h):
            size_p, size_s = (nx, ny) if h == 0 else (ny, nx)
            p, s = (x, y) if h == 0 else (y, x)

            def index(ss, pp):
                ss, pp = lax.rem(ss + 4, 4), lax.rem(pp + 4, 4)
                return ss * nx + pp if h == 0 else pp * nx + ss

            rel = (0, -1, 1, 2)
            whole, low, high = (0, rows), (0, quarter), (quarter, quarter)

            def msg(name, ds, dp, part):
                sem = {"pr": 0, "pl": 1, "fr": 2, "fl": 3}.get(name)
                if sem is None:
                    sem = 4 + 4 * ("su", "sd", "gu", "gd").index(name[:2]) + int(name[2])
                ts, tp_ = {
                    "pr": (0, 1), "pl": (0, -1), "fr": (0, 1), "fl": (0, -1),
                    "su": (1, 0), "sd": (-1, 0), "gu": (1, 0), "gd": (-1, 0),
                }[name if sem < 4 else name[:2]]
                ref = block(h, index(s + ds, p + dp), *part)
                return remote(
                    ref, ref, xy_send.at[number, h, sem], xy_recv.at[number, h, sem], {"tp": index(s + ts, p + tp_)}
                )

            sent = []

            def send(name, ds, dp, part):
                msg(name, ds, dp, part).start()
                sent.append(lambda: msg(name, ds, dp, part).wait_send())

            def prime():
                send("pr", 0, 0, whole)
                send("pl", 0, 0, whole)

            def out(j):
                send(f"su{j}", 0, rel[j], whole)
                send(f"sd{j}", 0, rel[j], whole)

            def across():
                msg("pr", 0, -1, whole).wait_recv()
                send("fr", 0, -1, low)
                msg("pl", 0, 1, whole).wait_recv()
                send("fl", 0, 1, high)

            def opposite():
                msg("fr", 0, -2, low).wait_recv()
                msg("fl", 0, 2, high).wait_recv()

            def forward(j):
                msg(f"su{j}", -1, rel[j], whole).wait_recv()
                send(f"gu{j}", -1, rel[j], low)
                msg(f"sd{j}", 1, rel[j], whole).wait_recv()
                send(f"gd{j}", 1, rel[j], high)

            def ended(j):
                msg(f"gu{j}", -2, rel[j], low).wait_recv()
                msg(f"gd{j}", 2, rel[j], high).wait_recv()

            steps_of = {
                0: [prime, lambda: out(0)],
                1: [across, lambda: (out(1), out(2))],
                2: [opposite, lambda: out(3)],
                5: [lambda: [ended(j) for j in range(4)]],
            }
            for j in range(4):
                steps_of[30 + j] = [functools.partial(forward, j)]
            return steps_of, sent

        if n_tp == 1:
            return lambda i: None, lambda: None
        (a, sent_a), (b, sent_b) = half_stages(0), half_stages(1)

        def both(i):
            with jax.named_scope(f"g{number}_{i}"):
                for one, two in zip(a[i], b[i]):
                    one()
                    two()

        def drained():
            for wait in sent_a + sent_b:
                wait()

        return both, drained

    passes = 2
    rows_p = slots // passes
    rows_x = rows_p // 2

    def x_block(p, h, owner, row, count):
        return xbuf.at[owner, pl.ds(p * rows_p + h * rows_x + row, count)]

    def h_block(p, h, owner, row, count):
        return hbuf.at[pl.ds(p * rows_p + h * rows_x + row, count), pl.ds(pl.multiple_of(owner * ff, 128), ff)]

    rows_a = ta // 2

    def ho_block(h, owner, row, count):
        return hobuf.at[pl.ds(h * rows_a + row, count), pl.ds(pl.multiple_of(owner * vd, 128), vd)]

    xs = [plane_gather(p, rows_x, functools.partial(x_block, p)) for p in range(passes)]
    hs = [plane_gather(passes + p, rows_x, functools.partial(h_block, p)) for p in range(passes)]
    o_stage, o_sent = plane_gather(2 * passes, rows_a, ho_block)

    def add_group(p, h, ds):
        at = slice(p * rows_p + h * rows_x, p * rows_p + (h + 1) * rows_x)
        if n_tp == 1:
            owners = [0]
        elif h == 0:
            owners = [lax.rem(y + ds + ny, ny) * nx + j for j in range(nx)]
        else:
            owners = [j * nx + lax.rem(x + ds + nx, nx) for j in range(ny)]
        total, squares = gu[at, :], ssq[at, :]
        for owner in owners:
            rows = xbuf[owner, at, :]
            total = total + dot(rows, wgu[pl.ds(pl.multiple_of(owner * dcol, dcol), dcol), :])
            wide = rows.astype(F32)
            wide = wide * wide
            for j in range(dcol // 128):
                squares = squares + wide[:, 128 * j : 128 * (j + 1)]
        gu[at, :] = total
        ssq[at, :] = squares

    def x_stage(p, i):
        if i == 0:
            with jax.named_scope("disp_wait"):
                others(2 * nz // passes * p, 2 * nz // passes * (p + 1), lambda j: dispatched(j).wait_recv())
        xs[p][0](i)
        with jax.named_scope("gate_up"):
            for ds in {32: (0,), 5: (2,)}.get(i, ()) if n_tp > 1 else (0,) * (i == 5):
                for h in range(2):
                    add_group(p, h, ds)
        if i == 5:
            at = slice(p * rows_p, (p + 1) * rows_p)
            mean = jnp.sum(ssq[at, :], axis=1, keepdims=True) / (n_tp * dcol)
            both = gu[at, :] * lax.rsqrt(mean + EPS)
            gate, up = both[:, 0:ff], both[:, ff : 2 * ff]
            hidden = (gate / (1.0 + jnp.exp(-gate)) * up).astype(BF16)
            hbuf[at, pl.ds(pl.multiple_of(tp * ff, 128), ff)] = hidden
            hs[p][0](0)

    def h_stage(p, i):
        hs[p][0](i)
        if i == 5:
            at = slice(p * rows_p, (p + 1) * rows_p)
            if p == 0:
                w_copies[2].wait()
            with jax.named_scope("down"):
                obuf[at, :] = dot(hbuf[at, :], wdown[...]).astype(BF16)
            others(2 * nz // passes * p, 2 * nz // passes * (p + 1), lambda j: return_copy(j).start())
            if p == passes - 1:
                rbuf[rows_of(ep), :] = obuf[rows_of(self_place), :]

    def run(items):
        for what, p, i in items:
            if what == "sides":
                if n_tp > 1:
                    with jax.named_scope("gate_up"):
                        for ds in (-1, 1):
                            for h in range(2):
                                add_group(p, h, ds)
            else:
                (x_stage if what == "x" else h_stage)(p, i)

    def use(core, s, lo, hi):
        _, used = comes(core, s)

        @pl.when(used & (s >= 1))
        def _():
            if lo == 0:

                @pl.when(c != core)
                def _():
                    with jax.named_scope("handed"):
                        for e in range(4):
                            handed(s, e).wait_recv()

            with jax.named_scope("attend"):
                loop(lo, hi, lambda n: attend(owner_of(core, s), n, False))

    run(PLAN[0])
    split = tiles - tiles // 3

    def tick(s):
        for e in range(4):
            with jax.named_scope("ring"):
                ring_event(s, e)
            for at, items in PLAN[1].items():
                if at % 4 == e and at // 4 + 1 <= steps + 1:
                    pl.when(s == at // 4 + 1)(functools.partial(run, items))
            use(e // 2, s - 1, *((0, split), (split, tiles))[e % 2])

    loop(1, steps + 2, tick)
    for at, items in PLAN[1].items():
        if at // 4 + 1 > steps + 1:
            run(items)

    def sent_so_far():
        for e in range(2):
            handover(0, e).wait_send()

        def drain(s):
            _, used = comes(c, s)
            for e in range(4):
                pl.when(goes(s))(lambda e=e: hop(s, e).wait_send())
                pl.when(used)(lambda e=e: handover(s, e).wait_send())

        loop(1, steps + 1, drain)
        others(0, n_ep, lambda i: dispatch_copy(i).wait_send())
        for _, sent in xs + hs:
            sent()

    maps = acc[0:vd, :] / acc[vd : vd + 1, :]
    mixed = maps[:, 0:ta] - scale_ref[0] * maps[:, ta : 2 * ta]
    mean_sq = jnp.mean(mixed * mixed, axis=0, keepdims=True)
    head = (mixed * lax.rsqrt(mean_sq + EPS)).T * hgain_ref[...] * HEAD_FACTOR
    hobuf[:, pl.ds(pl.multiple_of(tp * vd, 128), vd)] = head.astype(BF16)
    o_stage(0)

    sent_so_far()
    for i in (1, 30, 2, 31, 32, 33, 5):
        o_stage(i)
    w_copies[3].wait()
    with jax.named_scope("outproj"):
        mixer_ref[...] = dot(hobuf[...], wout[...]).astype(BF16)

    def other_experts(f):
        loop(1, n_ep, lambda i: f(lax.rem(ep + i, n_ep)))

    with jax.named_scope("ret_wait"):
        other_experts(lambda peer: returned(peer).wait_recv())
    back = rbuf[...]
    weight = [column(rw_ref[i : i + 1, :])[:, 0:1] for i in range(2)]
    mix_ref[...] = (dot(picks[0], back) * weight[0] + dot(picks[1], back) * weight[1]).astype(BF16)

    others(0, n_ep, lambda i: return_copy(i).wait_send())
    o_sent()


def per_device(nz, ny, nx, *args):
    q, k, v, scale, hgain, wout, x, ngain, ids, rw, gate, up, down = args
    ta, hd2 = q.shape
    vd = v.shape[1]
    tb, dcol = x.shape
    n_ep, n_tp = 2 * nz, ny * nx
    cap = 2 * tb * ids.shape[1] // n_ep
    slots = n_ep * cap
    d, ff = gate.shape[1:]
    gate, up, down = gate.reshape(d, ff), up.reshape(d, ff), down.reshape(down.shape[1:])
    ocol = down.shape[1]
    steps = nz // 2
    vmem = pl.BlockSpec(memory_space=pltpu.VMEM)
    hbm = pl.BlockSpec(memory_space=pl.ANY)
    dma = pltpu.SemaphoreType.DMA
    return pl.pallas_call(
        functools.partial(kernel, nz, ny, nx, cap),
        out_shape=(
            jax.ShapeDtypeStruct((ta, wout.shape[1]), BF16),
            jax.ShapeDtypeStruct((tb, ocol), BF16),
        ),
        in_specs=[
            vmem, vmem, vmem, pl.BlockSpec(memory_space=pltpu.SMEM), vmem, hbm, vmem, vmem, vmem, vmem, hbm, hbm, hbm,
        ],
        out_specs=(vmem, vmem),
        scratch_shapes=[
            pltpu.VMEM((n_ep, ta, hd2), BF16),
            pltpu.VMEM((nz, vd + 16, 2 * ta), BF16),
            pltpu.VMEM((2 * hd2, 2 * ta), BF16),
            pltpu.VMEM((1, 2 * ta), F32),
            pltpu.VMEM((vd + 16, 2 * ta), F32),
            pltpu.VMEM((d // 128, 128), F32),
            pltpu.VMEM((slots, 128), F32),
            pltpu.VMEM((slots, dcol), BF16),
            pltpu.VMEM((n_tp, slots, dcol), BF16),
            pltpu.VMEM((slots, 2 * ff), F32),
            pltpu.VMEM((slots, n_tp * ff), BF16),
            pltpu.VMEM((slots, ocol), BF16),
            pltpu.VMEM((slots, ocol), BF16),
            pltpu.VMEM((ta, n_tp * vd), BF16),
            pltpu.VMEM((2, tb, slots), BF16),
            pltpu.VMEM((d, 2 * ff), BF16),
            pltpu.VMEM(down.shape, BF16),
            pltpu.VMEM(wout.shape, BF16),
            dma((4,)),
            dma((steps + 1, 4)),
            dma((steps + 1, 4)),
            dma((steps + 1, 4)),
            dma((steps + 1, 4)),
            dma((2, n_ep)),
            dma((2, n_ep)),
            dma((5, 2, 20)),
            dma((5, 2, 20)),
        ],
        compiler_params=pltpu.CompilerParams(
            collective_id=0, has_side_effects=True, vmem_limit_bytes=60 * 1024 * 1024
        ),
        name="layer",
    )(q, k, v, scale, hgain.reshape(1, -1), wout, x, ngain.reshape(1, -1), ids.T, rw.T, gate, up, down)


def solution(mesh):
    placed = (
        P("ep", "tp"),
        P("ep", "tp"),
        P("ep", "tp"),
        P("tp"),
        P(),
        P(None, "tp"),
        P("ep", "tp"),
        P(),
        P("ep", None),
        P("ep", None),
        P("ep", None, "tp"),
        P("ep", None, "tp"),
        P("ep", None, "tp"),
    )
    ny, nx = PLANE[mesh.shape["tp"]]
    return jax.shard_map(
        functools.partial(per_device, mesh.shape["ep"] // 2, ny, nx),
        mesh=mesh,
        in_specs=placed,
        out_specs=(P("ep", "tp"), P("ep", "tp")),
        check_vma=False,
    )
```

```python
import functools
import math

import jax
import jax.numpy as jnp
from jax import lax
from jax.experimental import pallas as pl
from jax.experimental.pallas import tpu as pltpu
from jax.sharding import PartitionSpec as P

MESH = pl.DeviceIdType.MESH
F32 = jnp.float32
BF16 = jnp.bfloat16
EPS = 1e-06
HEAD_FACTOR = 0.8
NEG = -1e30
PLANE = {16: (4, 4), 1: (1, 1)}
PLAN = (
    [("x", 0, 0), ("x", 0, 10), ("x", 1, 0)],
    {
        2: [("x", 0, 1), ("x", 0, 11)],
        3: [("x", 0, 30)],
        5: [("x", 1, 1), ("x", 0, 12), ("x", 0, 2)],
        6: [("x", 1, 11), ("x", 1, 10)],
        9: [("x", 0, 32)],
        11: [("x", 0, 33), ("x", 0, 31), ("sides", 0, 0), ("x", 1, 2), ("x", 1, 12)],
        13: [("x", 1, 30)],
        15: [("x", 0, 5)],
        17: [("x", 1, 33), ("x", 1, 31)],
        18: [("x", 1, 32), ("sides", 1, 0)],
        19: [("h", 0, 1)],
        20: [("h", 0, 11), ("h", 0, 10), ("h", 0, 12)],
        21: [("x", 1, 5)],
        22: [("h", 0, 2)],
        23: [("h", 0, 30)],
        24: [("h", 0, 31), ("h", 0, 32)],
        25: [("h", 0, 33)],
        26: [("h", 1, 1), ("h", 1, 12), ("h", 1, 10), ("h", 1, 11)],
        28: [("h", 0, 5)],
        29: [("h", 1, 2)],
        30: [("h", 1, 30), ("h", 1, 31)],
        31: [("h", 1, 32), ("h", 1, 33)],
    },
    [("o", 0, 0), ("o", 0, 10), ("h", 1, 5), ("o", 0, 1), ("o", 0, 12), ("o", 0, 11), ("o", 0, 2), ("o", 0, 32), ("o", 0, 30), ("o", 0, 31), ("o", 0, 33), ("o", 0, 5)],
)


def dot(a, b):
    return lax.dot_general(a, b, (((1,), (0,)), ((), ())), preferred_element_type=F32)


def kernel(
    nz,
    ny,
    nx,
    cap,
    q_ref,
    k_ref,
    v_ref,
    scale_ref,
    hgain_ref,
    wout_hbm,
    x_ref,
    ngain_ref,
    ids_ref,
    rw_ref,
    gate_hbm,
    up_hbm,
    down_hbm,
    mixer_ref,
    mix_ref,
    kbuf,
    vbuf,
    qq,
    m_ref,
    acc,
    gs,
    ssq,
    disp,
    xbuf,
    gu,
    hbuf,
    obuf,
    rbuf,
    hobuf,
    picks,
    wgu,
    wdown,
    wout,
    w_sem,
    ring_send,
    ring_recv,
    pass_send,
    pass_recv,
    a2a_send,
    a2a_recv,
    xy_send,
    xy_recv,
):
    n_ep, n_tp = 2 * nz, ny * nx
    ta, hd2 = q_ref.shape
    vd = v_ref.shape[1]
    tb, dcol = x_ref.shape
    slots = n_ep * cap
    ff = gate_hbm.shape[1]
    ocol = wdown.shape[1]
    steps = nz // 2

    ep = lax.axis_index("ep")
    tp = lax.axis_index("tp")
    z, c = lax.div(ep, 2), lax.rem(ep, 2)
    y, x = lax.div(tp, nx), lax.rem(tp, nx)

    def at_ep(zz, cc):
        return {"ep": 2 * zz + cc}

    def remote(src, dst, ssem, rsem, dev):
        return pltpu.make_async_remote_copy(
            src_ref=src, dst_ref=dst, send_sem=ssem, recv_sem=rsem, device_id=dev, device_id_type=MESH
        )

    barrier = pltpu.get_barrier_semaphore()

    def greet_ep(i, carry):
        pl.semaphore_signal(barrier, inc=1, device_id={"ep": lax.rem(ep + i, n_ep)}, device_id_type=MESH)
        return carry

    def greet_tp(i, carry):
        pl.semaphore_signal(barrier, inc=1, device_id={"tp": lax.rem(tp + i, n_tp)}, device_id_type=MESH)
        return carry

    lax.fori_loop(1, n_ep, greet_ep, 0)
    if n_tp > 1:
        lax.fori_loop(1, n_tp, greet_tp, 0)

    w_copies = [
        pltpu.make_async_copy(gate_hbm, wgu.at[:, pl.ds(0, ff)], w_sem.at[0]),
        pltpu.make_async_copy(up_hbm, wgu.at[:, pl.ds(ff, ff)], w_sem.at[1]),
        pltpu.make_async_copy(down_hbm, wdown, w_sem.at[2]),
        pltpu.make_async_copy(wout_hbm, wout, w_sem.at[3]),
    ]
    for copy in w_copies:
        copy.start()

    v_t = v_ref[...].astype(F32).T.astype(BF16)

    @pl.when(c == 0)
    def _():
        vbuf[z, 0:vd, 0:ta] = v_t

    @pl.when(c == 1)
    def _():
        vbuf[z, 0:vd, ta : 2 * ta] = v_t

    kbuf[ep] = k_ref[...]

    def ones_rows(i, carry):
        vbuf[i, vd : vd + 16, :] = jnp.ones((16, 2 * ta), BF16)
        return carry

    lax.fori_loop(0, nz, ones_rows, 0)

    half = hd2 // 2
    q_t = (q_ref[...].astype(F32) * (math.log2(math.e) * half**-0.5)).T
    q_hi = q_t.astype(BF16)
    q_lo = (q_t - q_hi.astype(F32)).astype(BF16)
    none = jnp.zeros((half, ta), BF16)
    for i, part in enumerate((q_hi, q_lo)):
        qq[2 * half * i : 2 * half * i + half, 0:ta] = part[0:half]
        qq[2 * half * i : 2 * half * i + half, ta : 2 * ta] = none
        qq[2 * half * i + half : 2 * half * (i + 1), 0:ta] = none
        qq[2 * half * i + half : 2 * half * (i + 1), ta : 2 * ta] = part[half:]
    m_ref[...] = jnp.full(m_ref.shape, NEG, F32)
    acc[...] = jnp.zeros(acc.shape, F32)
    gu[...] = jnp.zeros(gu.shape, F32)
    ssq[...] = jnp.zeros(ssq.shape, F32)
    for i in range(gs.shape[0]):
        gs[i : i + 1, :] = ngain_ref[:, 128 * i : 128 * (i + 1)]

    def column(row):
        return jnp.broadcast_to(row, (128, tb)).T

    ids = [column(ids_ref[i : i + 1, :].astype(F32)) for i in range(2)]
    lane = lax.broadcasted_iota(jnp.int32, (tb, 128), 1).astype(F32)
    first = jnp.where(ids[0] == lane, 1.0, 0.0).astype(F32)
    second = jnp.where(ids[1] == lane, 1.0, 0.0).astype(F32)
    lower = jnp.where(
        lax.broadcasted_iota(jnp.int32, (tb, tb), 0) > lax.broadcasted_iota(jnp.int32, (tb, tb), 1), 1.0, 0.0
    ).astype(BF16)
    before_0 = dot(lower, first.astype(BF16))
    before_1 = dot(lower, second.astype(BF16)) + jnp.sum(first, axis=0, keepdims=True)
    rank_0 = jnp.sum(first * before_0, axis=1, keepdims=True)
    rank_1 = jnp.sum(second * before_1, axis=1, keepdims=True)
    slot_0 = ids[0][:, 0:1] * cap + rank_0
    slot_1 = ids[1][:, 0:1] * cap + rank_1
    slot_lane = lax.broadcasted_iota(jnp.int32, (tb, slots), 1).astype(F32)
    pick_0 = jnp.where(slot_0 == slot_lane, 1.0, 0.0).astype(F32)
    pick_1 = jnp.where(slot_1 == slot_lane, 1.0, 0.0).astype(F32)
    picks[0] = pick_0.astype(BF16)
    picks[1] = pick_1.astype(BF16)
    disp[...] = dot((pick_0 + pick_1).T.astype(BF16), x_ref[...]).astype(BF16)

    with jax.named_scope("barrier"):
        pl.semaphore_wait(barrier, (n_ep - 1) + (n_tp - 1))

    def loop(lo, hi, f):
        if not isinstance(lo, int) or not isinstance(hi, int) or hi > lo:
            lax.fori_loop(lo, hi, lambda i, carry: (f(i), carry)[1], 0)

    passes = 2

    def chip_at(k):
        away = steps - lax.div(k + 1, 2)
        return lax.rem(jnp.where(lax.rem(k, 2) == 1, z + away, z - away + nz), nz)

    def mirrored(k):
        swapped = jnp.where(lax.rem(k, 2) == 1, k + 1, k - 1)
        return jnp.where(jnp.logical_or(k == 0, k == nz - 1), k, swapped)

    def rows_of(i):
        return pl.ds(pl.multiple_of(i * cap, cap), cap)

    def dispatch_copy(i):
        k, core = lax.div(i, 2), lax.rem(i, 2)
        peer = 2 * chip_at(k) + core
        there = 2 * mirrored(k) + c
        group = lax.div(there, n_ep // passes)
        return remote(disp.at[rows_of(peer)], xbuf.at[tp, rows_of(there)], a2a_send.at[0], a2a_recv.at[group], {"ep": peer})

    def wait_for(ref, sem):
        pltpu.make_async_copy(ref, ref, sem).wait()

    def dispatched(p):
        each = n_ep // passes
        if nz == 1:
            pl.when(c != p)(lambda: wait_for(xbuf.at[0, pl.ds(0, cap)], a2a_recv.at[p]))
        else:
            wait_for(xbuf.at[0, pl.ds(0, (each - (p == passes - 1)) * cap)], a2a_recv.at[p])

    def return_copy(i):
        peer = 2 * chip_at(lax.div(i, 2)) + lax.rem(i, 2)
        return remote(obuf.at[rows_of(i)], rbuf.at[rows_of(ep)], a2a_send.at[1], a2a_recv.at[passes], {"ep": peer})

    all_but_one = pl.ds(0, (n_ep - 1) * cap)

    self_place = 2 * (nz - 1) + c

    def others(lo, hi, f):
        def each(i):
            pl.when(i != self_place)(lambda: f(i))

        loop(lo, hi, each)

    others(0, n_ep, lambda i: dispatch_copy(i).start())
    xbuf[tp, rows_of(self_place), :] = disp[rows_of(ep), :]

    def k_at(zz, cc):
        return kbuf.at[2 * zz + cc]

    def v_at(zz, cc):
        return vbuf.at[zz, pl.ds(0, vd), pl.ds(pl.multiple_of(cc * ta, 128), ta)]

    def part(owner, core, e):
        return (k_at, v_at)[e % 2](owner, core if e < 2 else 1 - core)

    last = jnp.where(c == 0, steps, nz - 1 - steps)
    next_chip = jnp.where(c == 0, lax.rem(z + 1, nz), lax.rem(z - 1 + nz, nz))

    def owner_of(core, s):
        return lax.rem(jnp.where(core == 0, z - s + nz, z + s), nz)

    def comes(core, s):
        low = nz - 2 - steps
        up, down = z - s >= 0, z + s - nz >= 0
        brought = jnp.where(core == 0, up & (s <= steps), (owner_of(core, s) <= low) & (s <= low + 1))
        return brought, brought & ((core == 0) | down)

    def goes(s):
        low = nz - 2 - steps
        return jnp.where(
            c == 0,
            (z + 1 < nz) & (z - (s - 1) >= 0) & (s <= steps),
            (owner_of(c, s - 1) <= low) & (s <= low + 1),
        )

    def hop(s, e):
        ref = part(owner_of(c, s - 1), c, e)
        return remote(ref, ref, ring_send.at[s], ring_recv.at[s, e], at_ep(next_chip, c))

    def hopped(s, e):
        ref = part(owner_of(c, s), c, e)
        return remote(ref, ref, ring_send.at[s], ring_recv.at[s, e], at_ep(next_chip, c))

    def handover(s, e):
        ref = part(owner_of(c, s), c, e)
        return remote(ref, ref, pass_send.at[s], pass_recv.at[s], at_ep(z, 1 - c))

    def chunks(n):
        return kbuf.at[pl.ds(0, min(n, n_ep))]

    for e in range(2):
        pl.when(goes(1))(lambda e=e: hop(1, e).start())
        handover(0, e).start()

    def ring_event(s, e):
        brought, used = comes(c, s)

        @pl.when(brought)
        def _():
            hopped(s, e).wait_recv()
            pl.when(goes(s + 1))(lambda: hop(s + 1, e).start())
            pl.when(used)(lambda: handover(s, e).start())

    n_tile = 256 if (2 * ta) % 256 == 0 else 2 * ta
    tiles = 2 * ta // n_tile

    def attend(owner, masked):
        keys = kbuf[pl.ds(2 * owner, 2)].reshape(2 * ta, hd2)
        keys = jnp.concatenate([keys, keys], axis=1)

        def scores(n):
            return dot(keys, qq[:, n * n_tile : (n + 1) * n_tile])

        ahead = scores(0)
        for n in range(tiles):
            s, cols = ahead, slice(n * n_tile, (n + 1) * n_tile)
            if n + 1 < tiles:
                ahead = scores(n + 1)
            if masked:
                row = lax.broadcasted_iota(jnp.int32, s.shape, 0)
                col = lax.broadcasted_iota(jnp.int32, s.shape, 1) + n * n_tile
                col = jnp.where(col >= ta, col - ta, col) + c * ta
                s = jnp.where(row <= col, s, NEG)
            old = m_ref[:, cols]
            new = jnp.maximum(old, jnp.max(s, axis=0, keepdims=True))
            weights = jnp.exp2(s - new).astype(BF16)
            shrink = jnp.exp2(old - new)
            m_ref[:, cols] = new
            acc[:, cols] = acc[:, cols] * shrink + dot(vbuf[owner], weights)

    with jax.named_scope("own_wait"):
        wait_for(chunks(2), pass_recv.at[0])
        for e in range(2, 4):
            pl.when(goes(1))(lambda e=e: hop(1, e).start())
    with jax.named_scope("own_attend"):
        attend(z, True)

    with jax.named_scope("gain"):
        w_copies[0].wait()
        w_copies[1].wait()
        gain = gs[...].T
        for i in range(gs.shape[0]):
            rows = slice(128 * i, 128 * (i + 1))
            wgu[rows, :] = (wgu[rows, :].astype(F32) * gain[:, i : i + 1]).astype(BF16)

    def plane_gather(number, rows, block, span):
        quarter = rows // 2

        def half_stages(h):
            size_p, size_s = (nx, ny) if h == 0 else (ny, nx)
            p, s = (x, y) if h == 0 else (y, x)

            def index(ss, pp):
                ss, pp = lax.rem(ss + 4, 4), lax.rem(pp + 4, 4)
                return ss * nx + pp if h == 0 else pp * nx + ss

            rel = (0, -1, 1, 2)
            whole, low, high = (0, rows), (0, quarter), (quarter, quarter)

            def send(name, ds, dp, part):
                group = {"p": 0, "f": 1, "s": 2, "g": 6}[name[0]] + (int(name[2]) if name[0] == "s" else 0)
                ts, tp_ = {"r": (0, 1), "l": (0, -1), "u": (1, 0), "d": (-1, 0)}[name[1]]
                ref = block(h, index(s + ds, p + dp), *part)
                remote(
                    ref, ref, xy_send.at[number], xy_recv.at[number, group], {"tp": index(s + ts, p + tp_)}
                ).start()

            def prime():
                send("pr", 0, 0, whole)
                send("pl", 0, 0, whole)

            def out(j):
                send(f"su{j}", 0, rel[j], whole)
                send(f"sd{j}", 0, rel[j], whole)

            def across():
                send("fr", 0, -1, low)
                send("fl", 0, 1, high)

            def forward(j):
                send("gu", -1, rel[j], low)
                send("gd", 1, rel[j], high)

            sends = {0: prime, 10: lambda: out(0), 1: across, 11: lambda: out(1), 12: lambda: out(2), 2: lambda: out(3)}
            for j in range(4):
                sends[30 + j] = functools.partial(forward, j)
            return sends

        if n_tp == 1:
            return lambda i: None, lambda: None
        first, second = half_stages(0), half_stages(1)
        waits = {1: (0, 4), 2: (1, 2), 30: (2, 4), 31: (3, 4), 32: (4, 4), 33: (5, 4), 5: (6, 8)}

        def both(i):
            with jax.named_scope(f"g{number}_{i}"):
                if i in waits:
                    kind, count = waits[i]
                    wait_for(span(count), xy_recv.at[number, kind])
                if i in first:
                    first[i]()
                    second[i]()

        def drained():
            wait_for(span(30), xy_send.at[number])

        return both, drained

    rows_p = slots // passes
    rows_x = rows_p // 2

    def x_block(p, h, owner, row, count):
        return xbuf.at[owner, pl.ds(p * rows_p + h * rows_x + row, count)]

    def h_block(p, h, owner, row, count):
        return hbuf.at[pl.ds(p * rows_p + h * rows_x + row, count), pl.ds(pl.multiple_of(owner * ff, 128), ff)]

    rows_a = ta // 2

    def ho_block(h, owner, row, count):
        return hobuf.at[pl.ds(h * rows_a + row, count), pl.ds(pl.multiple_of(owner * vd, 128), vd)]

    def x_span(n):
        return xbuf.at[pl.ds(0, n // 2), pl.ds(0, 2 * rows_x)]

    def h_span(n):
        return hbuf.at[pl.ds(0, 2 * rows_x), pl.ds(0, n // 2 * ff)]

    def ho_span(n):
        return hobuf.at[pl.ds(0, 2 * rows_a), pl.ds(0, n // 2 * vd)]

    xs = [plane_gather(p, rows_x, functools.partial(x_block, p), x_span) for p in range(passes)]
    hs = [plane_gather(passes + p, rows_x, functools.partial(h_block, p), h_span) for p in range(passes)]
    o_stage, o_sent = plane_gather(2 * passes, rows_a, ho_block, ho_span)

    def add_group(p, h, ds):
        at = slice(p * rows_p + h * rows_x, p * rows_p + (h + 1) * rows_x)
        if n_tp == 1:
            owners = [0]
        elif h == 0:
            owners = [lax.rem(y + ds + ny, ny) * nx + j for j in range(nx)]
        else:
            owners = [j * nx + lax.rem(x + ds + nx, nx) for j in range(ny)]
        total, squares = gu[at, :], ssq[at, :]
        for owner in owners:
            rows = xbuf[owner, at, :]
            total = total + dot(rows, wgu[pl.ds(pl.multiple_of(owner * dcol, dcol), dcol), :])
            wide = rows.astype(F32)
            wide = wide * wide
            for j in range(dcol // 128):
                squares = squares + wide[:, 128 * j : 128 * (j + 1)]
        gu[at, :] = total
        ssq[at, :] = squares

    def x_stage(p, i):
        if i == 0:
            with jax.named_scope("disp_wait"):
                dispatched(p)
        xs[p][0](i)
        with jax.named_scope("gate_up"):
            for ds in {32: (0,), 5: (2,)}.get(i, ()) if n_tp > 1 else (0,) * (i == 5):
                for h in range(2):
                    add_group(p, h, ds)
        if i == 5:
            at = slice(p * rows_p, (p + 1) * rows_p)
            mean = jnp.sum(ssq[at, :], axis=1, keepdims=True) / (n_tp * dcol)
            both = gu[at, :] * lax.rsqrt(mean + EPS)
            gate, up = both[:, 0:ff], both[:, ff : 2 * ff]
            hidden = (gate / (1.0 + jnp.exp(-gate)) * up).astype(BF16)
            hbuf[at, pl.ds(pl.multiple_of(tp * ff, 128), ff)] = hidden
            hs[p][0](0)

    def h_stage(p, i):
        hs[p][0](i)
        if i == 5:
            at = slice(p * rows_p, (p + 1) * rows_p)
            if p == 0:
                w_copies[2].wait()
            with jax.named_scope("down"):
                obuf[at, :] = dot(hbuf[at, :], wdown[...]).astype(BF16)
            others(2 * nz // passes * p, 2 * nz // passes * (p + 1), lambda j: return_copy(j).start())
            if p == passes - 1:
                rbuf[rows_of(ep), :] = obuf[rows_of(self_place), :]

    def run(items):
        for what, p, i in items:
            if what == "sides":
                if n_tp > 1:
                    with jax.named_scope("gate_up"):
                        for ds in (-1, 1):
                            for h in range(2):
                                add_group(p, h, ds)
            else:
                (x_stage if what == "x" else h_stage)(p, i)

    def use(core, s):
        _, used = comes(core, s)

        @pl.when(used & (s >= 1))
        def _():
            @pl.when(c != core)
            def _():
                with jax.named_scope("handed"):
                    wait_for(chunks(4), pass_recv.at[s])

            with jax.named_scope("attend"):
                attend(owner_of(core, s), False)

    run(PLAN[0])

    def tick(s):
        for e in range(4):
            with jax.named_scope("ring"):
                ring_event(s, e)
            for at, items in PLAN[1].items():
                if at % 4 == e and at // 4 + 1 <= steps + 1:
                    pl.when(s == at // 4 + 1)(functools.partial(run, items))
            if e % 2 == 0:
                use(e // 2, s - 1)

    loop(1, steps + 2, tick)
    for at, items in PLAN[1].items():
        if at // 4 + 1 > steps + 1:
            run(items)

    maps = acc[0:vd, :] / acc[vd : vd + 1, :]
    mixed = maps[:, 0:ta] - scale_ref[0] * maps[:, ta : 2 * ta]
    mean_sq = jnp.mean(mixed * mixed, axis=0, keepdims=True)
    head = (mixed * lax.rsqrt(mean_sq + EPS)).T * hgain_ref[...] * HEAD_FACTOR
    hobuf[:, pl.ds(pl.multiple_of(tp * vd, 128), vd)] = head.astype(BF16)

    for what, p, i in PLAN[2]:
        o_stage(i) if what == "o" else run([(what, p, i)])
    w_copies[3].wait()
    with jax.named_scope("outproj"):
        mixer_ref[...] = dot(hobuf[...], wout[...]).astype(BF16)

    with jax.named_scope("ret_wait"):
        wait_for(rbuf.at[all_but_one], a2a_recv.at[passes])
    back = rbuf[...]
    weight = [column(rw_ref[i : i + 1, :])[:, 0:1] for i in range(2)]
    mix_ref[...] = (dot(picks[0], back) * weight[0] + dot(picks[1], back) * weight[1]).astype(BF16)

    with jax.named_scope("drain"):
        wait_for(chunks(2), pass_send.at[0])

        def drain(s):
            _, used = comes(c, s)
            pl.when(goes(s))(lambda: wait_for(chunks(4), ring_send.at[s]))
            pl.when(used)(lambda: wait_for(chunks(4), pass_send.at[s]))

        loop(1, steps + 1, drain)
        for i in range(2):
            wait_for(disp.at[all_but_one], a2a_send.at[i])
        for _, sent in xs + hs:
            sent()
        o_sent()


def per_device(nz, ny, nx, *args):
    q, k, v, scale, hgain, wout, x, ngain, ids, rw, gate, up, down = args
    ta, hd2 = q.shape
    vd = v.shape[1]
    tb, dcol = x.shape
    n_ep, n_tp = 2 * nz, ny * nx
    cap = 2 * tb * ids.shape[1] // n_ep
    slots = n_ep * cap
    d, ff = gate.shape[1:]
    gate, up, down = gate.reshape(d, ff), up.reshape(d, ff), down.reshape(down.shape[1:])
    ocol = down.shape[1]
    steps = nz // 2
    vmem = pl.BlockSpec(memory_space=pltpu.VMEM)
    hbm = pl.BlockSpec(memory_space=pl.ANY)
    dma = pltpu.SemaphoreType.DMA
    return pl.pallas_call(
        functools.partial(kernel, nz, ny, nx, cap),
        out_shape=(
            jax.ShapeDtypeStruct((ta, wout.shape[1]), BF16),
            jax.ShapeDtypeStruct((tb, ocol), BF16),
        ),
        in_specs=[
            vmem, vmem, vmem, pl.BlockSpec(memory_space=pltpu.SMEM), vmem, hbm, vmem, vmem, vmem, vmem, hbm, hbm, hbm,
        ],
        out_specs=(vmem, vmem),
        scratch_shapes=[
            pltpu.VMEM((n_ep, ta, hd2), BF16),
            pltpu.VMEM((nz, vd + 16, 2 * ta), BF16),
            pltpu.VMEM((2 * hd2, 2 * ta), BF16),
            pltpu.VMEM((1, 2 * ta), F32),
            pltpu.VMEM((vd + 16, 2 * ta), F32),
            pltpu.VMEM((d // 128, 128), F32),
            pltpu.VMEM((slots, 128), F32),
            pltpu.VMEM((slots, dcol), BF16),
            pltpu.VMEM((n_tp, slots, dcol), BF16),
            pltpu.VMEM((slots, 2 * ff), F32),
            pltpu.VMEM((slots, n_tp * ff), BF16),
            pltpu.VMEM((slots, ocol), BF16),
            pltpu.VMEM((slots, ocol), BF16),
            pltpu.VMEM((ta, n_tp * vd), BF16),
            pltpu.VMEM((2, tb, slots), BF16),
            pltpu.VMEM((d, 2 * ff), BF16),
            pltpu.VMEM(down.shape, BF16),
            pltpu.VMEM(wout.shape, BF16),
            dma((4,)),
            dma((steps + 1,)),
            dma((steps + 1, 4)),
            dma((steps + 1,)),
            dma((steps + 1,)),
            dma((2,)),
            dma((3,)),
            dma((5,)),
            dma((5, 7)),
        ],
        compiler_params=pltpu.CompilerParams(
            collective_id=0, has_side_effects=True, vmem_limit_bytes=60 * 1024 * 1024
        ),
        name="layer",
    )(q, k, v, scale, hgain.reshape(1, -1), wout, x, ngain.reshape(1, -1), ids.T, rw.T, gate, up, down)


def solution(mesh):
    placed = (
        P("ep", "tp"),
        P("ep", "tp"),
        P("ep", "tp"),
        P("tp"),
        P(),
        P(None, "tp"),
        P("ep", "tp"),
        P(),
        P("ep", None),
        P("ep", None),
        P("ep", None, "tp"),
        P("ep", None, "tp"),
        P("ep", None, "tp"),
    )
    ny, nx = PLANE[mesh.shape["tp"]]
    return jax.shard_map(
        functools.partial(per_device, mesh.shape["ep"] // 2, ny, nx),
        mesh=mesh,
        in_specs=placed,
        out_specs=(P("ep", "tp"), P("ep", "tp")),
        check_vma=False,
    )
```

```python
import functools
import math

import jax
import jax.numpy as jnp
from jax import lax
from jax.experimental import pallas as pl
from jax.experimental.pallas import tpu as pltpu
from jax.sharding import PartitionSpec as P

MESH = pl.DeviceIdType.MESH
F32 = jnp.float32
BF16 = jnp.bfloat16
EPS = 1e-06
HEAD_FACTOR = 0.8
NEG = -1e30
PLANE = {16: (4, 4), 1: (1, 1)}
PLAN = (
    [("x", 0, 0), ("x", 0, 10), ("x", 1, 0)],
    {
        2: [("x", 0, 1), ("x", 0, 11)],
        3: [("x", 0, 30)],
        5: [("x", 1, 1), ("x", 0, 12), ("x", 0, 2)],
        6: [("x", 1, 11), ("x", 1, 10)],
        9: [("x", 0, 32)],
        11: [("x", 0, 33), ("x", 0, 31), ("sides", 0, 0), ("x", 1, 2), ("x", 1, 12)],
        13: [("x", 1, 30)],
        15: [("x", 0, 5)],
        17: [("x", 1, 33), ("x", 1, 31)],
        18: [("x", 1, 32), ("sides", 1, 0)],
        19: [("h", 0, 1)],
        20: [("h", 0, 11), ("h", 0, 10), ("h", 0, 12)],
        21: [("x", 1, 5)],
        22: [("h", 0, 2), ("e", 0, 0)],
        23: [("h", 0, 30)],
        24: [("h", 0, 31), ("h", 0, 32), ("e", 0, 10)],
        25: [("h", 0, 33), ("e", 0, 1)],
        26: [("h", 1, 1), ("h", 1, 12), ("h", 1, 10), ("h", 1, 11)],
        27: [("e", 0, 12)],
        28: [("h", 0, 5), ("e", 0, 11)],
        29: [("h", 1, 2), ("e", 0, 2)],
        30: [("h", 1, 30), ("h", 1, 31), ("e", 0, 30)],
        31: [("h", 1, 32), ("h", 1, 33), ("e", 0, 32), ("e", 0, 31)],
    },
    [("o", 0, 0), ("o", 0, 10), ("h", 1, 5), ("e", 0, 33), ("e", 0, 5), ("o", 0, 1), ("o", 0, 12), ("o", 0, 11), ("o", 0, 2), ("o", 0, 32), ("o", 0, 30), ("o", 0, 31), ("o", 0, 33), ("o", 0, 5)],
)


def dot(a, b):
    return lax.dot_general(a, b, (((1,), (0,)), ((), ())), preferred_element_type=F32)


def kernel(
    nz,
    ny,
    nx,
    cap,
    q_ref,
    k_ref,
    v_ref,
    scale_ref,
    hgain_ref,
    wout_hbm,
    x_ref,
    ngain_ref,
    ids_ref,
    rw_ref,
    gate_hbm,
    up_hbm,
    down_hbm,
    mixer_ref,
    mix_ref,
    kbuf,
    vbuf,
    qq,
    m_ref,
    acc,
    gs,
    ssq,
    disp,
    xbuf,
    gu,
    hbuf,
    obuf,
    rbuf,
    hobuf,
    picks,
    wgu,
    wdown,
    wout,
    w_sem,
    ring_send,
    ring_recv,
    pass_send,
    pass_recv,
    a2a_send,
    a2a_recv,
    xy_send,
    xy_recv,
):
    n_ep, n_tp = 2 * nz, ny * nx
    ta, hd2 = q_ref.shape
    vd = v_ref.shape[1]
    tb, dcol = x_ref.shape
    slots = n_ep * cap
    ff = gate_hbm.shape[1]
    ocol = wdown.shape[1]
    steps = nz // 2

    ep = lax.axis_index("ep")
    tp = lax.axis_index("tp")
    z, c = lax.div(ep, 2), lax.rem(ep, 2)
    y, x = lax.div(tp, nx), lax.rem(tp, nx)

    def at_ep(zz, cc):
        return {"ep": 2 * zz + cc}

    def remote(src, dst, ssem, rsem, dev):
        return pltpu.make_async_remote_copy(
            src_ref=src, dst_ref=dst, send_sem=ssem, recv_sem=rsem, device_id=dev, device_id_type=MESH
        )

    barrier = pltpu.get_barrier_semaphore()

    def greet_ep(i, carry):
        pl.semaphore_signal(barrier, inc=1, device_id={"ep": lax.rem(ep + i, n_ep)}, device_id_type=MESH)
        return carry

    def greet_tp(i, carry):
        pl.semaphore_signal(barrier, inc=1, device_id={"tp": lax.rem(tp + i, n_tp)}, device_id_type=MESH)
        return carry

    lax.fori_loop(1, n_ep, greet_ep, 0)
    if n_tp > 1:
        lax.fori_loop(1, n_tp, greet_tp, 0)

    w_copies = [
        pltpu.make_async_copy(gate_hbm, wgu.at[:, pl.ds(0, ff)], w_sem.at[0]),
        pltpu.make_async_copy(up_hbm, wgu.at[:, pl.ds(ff, ff)], w_sem.at[1]),
        pltpu.make_async_copy(down_hbm, wdown, w_sem.at[2]),
        pltpu.make_async_copy(wout_hbm, wout, w_sem.at[3]),
    ]
    for copy in w_copies:
        copy.start()

    v_t = v_ref[...].astype(F32).T.astype(BF16)

    @pl.when(c == 0)
    def _():
        vbuf[z, 0:vd, 0:ta] = v_t

    @pl.when(c == 1)
    def _():
        vbuf[z, 0:vd, ta : 2 * ta] = v_t

    kbuf[ep] = k_ref[...]

    def ones_rows(i, carry):
        vbuf[i, vd : vd + 16, :] = jnp.ones((16, 2 * ta), BF16)
        return carry

    lax.fori_loop(0, nz, ones_rows, 0)

    half = hd2 // 2
    q_t = (q_ref[...].astype(F32) * (math.log2(math.e) * half**-0.5)).T
    q_hi = q_t.astype(BF16)
    q_lo = (q_t - q_hi.astype(F32)).astype(BF16)
    none = jnp.zeros((half, ta), BF16)
    for i, part in enumerate((q_hi, q_lo)):
        qq[2 * half * i : 2 * half * i + half, 0:ta] = part[0:half]
        qq[2 * half * i : 2 * half * i + half, ta : 2 * ta] = none
        qq[2 * half * i + half : 2 * half * (i + 1), 0:ta] = none
        qq[2 * half * i + half : 2 * half * (i + 1), ta : 2 * ta] = part[half:]
    m_ref[...] = jnp.full(m_ref.shape, NEG, F32)
    acc[...] = jnp.zeros(acc.shape, F32)
    gu[...] = jnp.zeros(gu.shape, F32)
    ssq[...] = jnp.zeros(ssq.shape, F32)
    for i in range(gs.shape[0]):
        gs[i : i + 1, :] = ngain_ref[:, 128 * i : 128 * (i + 1)]

    def column(row):
        return jnp.broadcast_to(row, (128, tb)).T

    ids = [column(ids_ref[i : i + 1, :].astype(F32)) for i in range(2)]
    lane = lax.broadcasted_iota(jnp.int32, (tb, 128), 1).astype(F32)
    first = jnp.where(ids[0] == lane, 1.0, 0.0).astype(F32)
    second = jnp.where(ids[1] == lane, 1.0, 0.0).astype(F32)
    lower = jnp.where(
        lax.broadcasted_iota(jnp.int32, (tb, tb), 0) > lax.broadcasted_iota(jnp.int32, (tb, tb), 1), 1.0, 0.0
    ).astype(BF16)
    before_0 = dot(lower, first.astype(BF16))
    before_1 = dot(lower, second.astype(BF16)) + jnp.sum(first, axis=0, keepdims=True)
    rank_0 = jnp.sum(first * before_0, axis=1, keepdims=True)
    rank_1 = jnp.sum(second * before_1, axis=1, keepdims=True)
    slot_0 = ids[0][:, 0:1] * cap + rank_0
    slot_1 = ids[1][:, 0:1] * cap + rank_1
    slot_lane = lax.broadcasted_iota(jnp.int32, (tb, slots), 1).astype(F32)
    pick_0 = jnp.where(slot_0 == slot_lane, 1.0, 0.0).astype(F32)
    pick_1 = jnp.where(slot_1 == slot_lane, 1.0, 0.0).astype(F32)
    picks[0] = pick_0.astype(BF16)
    picks[1] = pick_1.astype(BF16)
    disp[...] = dot((pick_0 + pick_1).T.astype(BF16), x_ref[...]).astype(BF16)

    with jax.named_scope("barrier"):
        pl.semaphore_wait(barrier, (n_ep - 1) + (n_tp - 1))

    def loop(lo, hi, f):
        if not isinstance(lo, int) or not isinstance(hi, int) or hi > lo:
            lax.fori_loop(lo, hi, lambda i, carry: (f(i), carry)[1], 0)

    passes = 2

    def chip_at(k):
        away = steps - lax.div(k + 1, 2)
        return lax.rem(jnp.where(lax.rem(k, 2) == 1, z + away, z - away + nz), nz)

    def mirrored(k):
        swapped = jnp.where(lax.rem(k, 2) == 1, k + 1, k - 1)
        return jnp.where(jnp.logical_or(k == 0, k == nz - 1), k, swapped)

    def rows_of(i):
        return pl.ds(pl.multiple_of(i * cap, cap), cap)

    def dispatch_copy(i):
        k, core = lax.div(i, 2), lax.rem(i, 2)
        peer = 2 * chip_at(k) + core
        there = 2 * mirrored(k) + c
        group = lax.div(there, n_ep // passes)
        return remote(disp.at[rows_of(peer)], xbuf.at[tp, rows_of(there)], a2a_send.at[0], a2a_recv.at[group], {"ep": peer})

    def wait_for(ref, sem):
        pltpu.make_async_copy(ref, ref, sem).wait()

    def dispatched(p):
        each = n_ep // passes
        if nz == 1:
            pl.when(c != p)(lambda: wait_for(xbuf.at[0, pl.ds(0, cap)], a2a_recv.at[p]))
        else:
            wait_for(xbuf.at[0, pl.ds(0, (each - (p == passes - 1)) * cap)], a2a_recv.at[p])

    def return_copy(i):
        peer = 2 * chip_at(lax.div(i, 2)) + lax.rem(i, 2)
        return remote(obuf.at[rows_of(i)], rbuf.at[rows_of(ep)], a2a_send.at[1], a2a_recv.at[passes], {"ep": peer})

    all_but_one = pl.ds(0, (n_ep - 1) * cap)

    self_place = 2 * (nz - 1) + c

    def others(lo, hi, f):
        def each(i):
            pl.when(i != self_place)(lambda: f(i))

        loop(lo, hi, each)

    others(0, n_ep, lambda i: dispatch_copy(i).start())
    xbuf[tp, rows_of(self_place), :] = disp[rows_of(ep), :]

    def k_at(zz, cc):
        return kbuf.at[2 * zz + cc]

    def v_at(zz, cc):
        return vbuf.at[zz, pl.ds(0, vd), pl.ds(pl.multiple_of(cc * ta, 128), ta)]

    def part(owner, core, e):
        return (k_at, v_at)[e % 2](owner, core if e < 2 else 1 - core)

    next_chip = jnp.where(c == 1, lax.rem(z + 1, nz), lax.rem(z - 1 + nz, nz))

    def owner_of(core, s):
        return lax.rem(jnp.where(core == 1, z - s + nz, z + s), nz)

    def comes(core, s):
        low = nz - 2 - steps
        up, down = z - s >= 0, z + s - nz >= 0
        brought = jnp.where(core == 1, up & (s <= steps), (owner_of(core, s) <= low) & (s <= low + 1))
        return brought, brought & ((core == 1) | down)

    def goes(s):
        low = nz - 2 - steps
        return jnp.where(
            c == 1,
            (z + 1 < nz) & (z - (s - 1) >= 0) & (s <= steps),
            (owner_of(c, s - 1) <= low) & (s <= low + 1),
        )

    def hop(s, e):
        ref = part(owner_of(c, s - 1), c, e)
        return remote(ref, ref, ring_send.at[s], ring_recv.at[s, e], at_ep(next_chip, c))

    def hopped(s, e):
        ref = part(owner_of(c, s), c, e)
        return remote(ref, ref, ring_send.at[s], ring_recv.at[s, e], at_ep(next_chip, c))

    def handover(s, e):
        ref = part(owner_of(c, s), c, e)
        return remote(ref, ref, pass_send.at[s], pass_recv.at[s], at_ep(z, 1 - c))

    def chunks(n):
        return kbuf.at[pl.ds(0, min(n, n_ep))]

    for e in range(2):
        pl.when(goes(1))(lambda e=e: hop(1, e).start())
        handover(0, e).start()

    def ring_event(s, e):
        brought, used = comes(c, s)

        @pl.when(brought)
        def _():
            hopped(s, e).wait_recv()
            pl.when(goes(s + 1))(lambda: hop(s + 1, e).start())
            pl.when(used)(lambda: handover(s, e).start())

    n_tile = 256 if (2 * ta) % 256 == 0 else 2 * ta
    tiles = 2 * ta // n_tile

    def attend(owner, masked):
        keys = kbuf[pl.ds(2 * owner, 2)].reshape(2 * ta, hd2)
        keys = jnp.concatenate([keys, keys], axis=1)

        def scores(n):
            return dot(keys, qq[:, n * n_tile : (n + 1) * n_tile])

        ahead = scores(0)
        for n in range(tiles):
            s, cols = ahead, slice(n * n_tile, (n + 1) * n_tile)
            if n + 1 < tiles:
                ahead = scores(n + 1)
            if masked:
                row = lax.broadcasted_iota(jnp.int32, s.shape, 0)
                col = lax.broadcasted_iota(jnp.int32, s.shape, 1) + n * n_tile
                col = jnp.where(col >= ta, col - ta, col) + c * ta
                s = jnp.where(row <= col, s, NEG)
            old = m_ref[:, cols]
            new = jnp.maximum(old, jnp.max(s, axis=0, keepdims=True))
            weights = jnp.exp2(s - new).astype(BF16)
            shrink = jnp.exp2(old - new)
            m_ref[:, cols] = new
            acc[:, cols] = acc[:, cols] * shrink + dot(vbuf[owner], weights)

    with jax.named_scope("own_wait"):
        wait_for(chunks(2), pass_recv.at[0])
        for e in range(2, 4):
            pl.when(goes(1))(lambda e=e: hop(1, e).start())
    with jax.named_scope("own_attend"):
        attend(z, True)

    with jax.named_scope("gain"):
        w_copies[0].wait()
        w_copies[1].wait()
        w_copies[2].wait()
        gain = gs[...].T
        for i in range(gs.shape[0]):
            rows = slice(128 * i, 128 * (i + 1))
            wgu[rows, :] = (wgu[rows, :].astype(F32) * gain[:, i : i + 1]).astype(BF16)

    def plane_gather(number, rows, block, span, direct=False):
        quarter = rows // 2

        def half_stages(h):
            size_p, size_s = (nx, ny) if h == 0 else (ny, nx)
            p, s = (x, y) if h == 0 else (y, x)

            def index(ss, pp):
                ss, pp = lax.rem(ss + 4, 4), lax.rem(pp + 4, 4)
                return ss * nx + pp if h == 0 else pp * nx + ss

            rel = (0, -1, 1, 2)
            whole, low, high = (0, rows), (0, quarter), (quarter, quarter)

            def send(name, ds, dp, part):
                group = {"p": 0, "f": 1, "s": 2, "g": 6}[name[0]] + (int(name[2]) if name[0] == "s" else 0)
                ts, tp_ = {"r": (0, 1), "l": (0, -1), "o": (0, 2), "u": (1, 0), "d": (-1, 0)}[name[1]]
                ref = block(h, index(s + ds, p + dp), *part)
                remote(
                    ref, ref, xy_send.at[number], xy_recv.at[number, group], {"tp": index(s + ts, p + tp_)}
                ).start()

            def prime():
                if direct:
                    send("fo", 0, 0, whole)
                send("pr", 0, 0, whole)
                send("pl", 0, 0, whole)

            def out(j):
                send(f"su{j}", 0, rel[j], whole)
                send(f"sd{j}", 0, rel[j], whole)

            def across():
                if not direct:
                    send("fr", 0, -1, low)
                    send("fl", 0, 1, high)

            def forward(j):
                send("gu", -1, rel[j], low)
                send("gd", 1, rel[j], high)

            sends = {0: prime, 10: lambda: out(0), 1: across, 11: lambda: out(1), 12: lambda: out(2), 2: lambda: out(3)}
            for j in range(4):
                sends[30 + j] = functools.partial(forward, j)
            return sends

        if n_tp == 1:
            return lambda i: None, lambda: None
        first, second = half_stages(0), half_stages(1)
        waits = {1: (0, 4), 2: (1, 2), 30: (2, 4), 31: (3, 4), 32: (4, 4), 33: (5, 4), 5: (6, 8)}

        def both(i):
            with jax.named_scope(f"g{number}_{i}"):
                if i in waits:
                    kind, count = waits[i]
                    wait_for(span(count), xy_recv.at[number, kind])
                if i in first:
                    first[i]()
                    second[i]()

        def drained():
            wait_for(span(30), xy_send.at[number])

        return both, drained

    rows_p = slots // passes
    rows_x = rows_p // 2

    def x_block(p, h, owner, row, count):
        return xbuf.at[owner, pl.ds(p * rows_p + h * rows_x + row, count)]

    def h_block(p, h, owner, row, count):
        return hbuf.at[pl.ds(p * rows_p + h * rows_x + row, count), pl.ds(pl.multiple_of(owner * ff, 128), ff)]

    rows_a = ta // 2

    def ho_block(h, owner, row, count):
        return hobuf.at[pl.ds(h * rows_a + row, count), pl.ds(pl.multiple_of(owner * vd, 128), vd)]

    def x_span(n):
        return xbuf.at[pl.ds(0, n // 2), pl.ds(0, 2 * rows_x)]

    def h_span(n):
        return hbuf.at[pl.ds(0, 2 * rows_x), pl.ds(0, n // 2 * ff)]

    def ho_span(n):
        return hobuf.at[pl.ds(0, 2 * rows_a), pl.ds(0, n // 2 * vd)]

    xs = [plane_gather(p, rows_x, functools.partial(x_block, p), x_span) for p in range(passes)]
    hs = [plane_gather(passes + p, rows_x, functools.partial(h_block, p), h_span, True) for p in range(passes)]
    o_stage, o_sent = plane_gather(2 * passes, rows_a, ho_block, ho_span, True)

    def add_group(p, h, ds):
        at = slice(p * rows_p + h * rows_x, p * rows_p + (h + 1) * rows_x)
        if n_tp == 1:
            owners = [0]
        elif h == 0:
            owners = [lax.rem(y + ds + ny, ny) * nx + j for j in range(nx)]
        else:
            owners = [j * nx + lax.rem(x + ds + nx, nx) for j in range(ny)]
        total, squares = gu[at, :], ssq[at, :]
        for owner in owners:
            rows = xbuf[owner, at, :]
            total = total + dot(rows, wgu[pl.ds(pl.multiple_of(owner * dcol, dcol), dcol), :])
            wide = rows.astype(F32)
            wide = wide * wide
            for j in range(dcol // 128):
                squares = squares + wide[:, 128 * j : 128 * (j + 1)]
        gu[at, :] = total
        ssq[at, :] = squares

    def x_stage(p, i):
        if i == 0:
            with jax.named_scope("disp_wait"):
                dispatched(p)
        xs[p][0](i)
        with jax.named_scope("gate_up"):
            for ds in {32: (0,), 5: (2,)}.get(i, ()) if n_tp > 1 else (0,) * (i == 5):
                for h in range(2):
                    add_group(p, h, ds)
        if i == 5:
            at = slice(p * rows_p, (p + 1) * rows_p)
            mean = jnp.sum(ssq[at, :], axis=1, keepdims=True) / (n_tp * dcol)
            both = gu[at, :] * lax.rsqrt(mean + EPS)
            gate, up = both[:, 0:ff], both[:, ff : 2 * ff]
            hidden = (gate / (1.0 + jnp.exp(-gate)) * up).astype(BF16)
            hbuf[at, pl.ds(pl.multiple_of(tp * ff, 128), ff)] = hidden
            hs[p][0](0)

    def h_stage(p, i):
        hs[p][0](i)
        if i == 5:
            at = slice(p * rows_p, (p + 1) * rows_p)
            with jax.named_scope("down"):
                obuf[at, :] = dot(hbuf[at, :], wdown[...]).astype(BF16)
            others(2 * nz // passes * p, 2 * nz // passes * (p + 1), lambda j: return_copy(j).start())
            if p == passes - 1:
                rbuf[rows_of(ep), :] = obuf[rows_of(self_place), :]

    def heads(i):
        if i == 0:
            maps = acc[0:vd, :] / acc[vd : vd + 1, :]
            mixed = maps[:, 0:ta] - scale_ref[0] * maps[:, ta : 2 * ta]
            mean_sq = jnp.mean(mixed * mixed, axis=0, keepdims=True)
            head = (mixed * lax.rsqrt(mean_sq + EPS)).T * hgain_ref[...] * HEAD_FACTOR
            hobuf[:, pl.ds(pl.multiple_of(tp * vd, 128), vd)] = head.astype(BF16)
        o_stage(i)

    early = nz // 4

    def run(items):
        for what, p, i in items:
            if what == "sides":
                if n_tp > 1:
                    with jax.named_scope("gate_up"):
                        for ds in (-1, 1):
                            for h in range(2):
                                add_group(p, h, ds)
            elif what == "e":
                pl.when(z < early)(functools.partial(heads, i))
            elif what == "o":
                pl.when(z >= early)(functools.partial(heads, i))
            else:
                (x_stage if what == "x" else h_stage)(p, i)

    def use(core, s):
        _, used = comes(core, s)

        @pl.when(used & (s >= 1))
        def _():
            @pl.when(c != core)
            def _():
                with jax.named_scope("handed"):
                    wait_for(chunks(4), pass_recv.at[s])

            with jax.named_scope("attend"):
                attend(owner_of(core, s), False)

    run(PLAN[0])

    def tick(s):
        for e in range(4):
            with jax.named_scope("ring"):
                ring_event(s, e)
            for at, items in PLAN[1].items():
                if at % 4 == e and at // 4 + 1 <= steps + 1:
                    pl.when(s == at // 4 + 1)(functools.partial(run, items))
            if e % 2 == 0:
                use(e // 2, s - 1)

    loop(1, steps + 2, tick)
    for at, items in PLAN[1].items():
        if at // 4 + 1 > steps + 1:
            run(items)
    run(PLAN[2])

    w_copies[3].wait()
    with jax.named_scope("outproj"):
        mixer_ref[...] = dot(hobuf[...], wout[...]).astype(BF16)

    with jax.named_scope("ret_wait"):
        wait_for(rbuf.at[all_but_one], a2a_recv.at[passes])
    back = rbuf[...]
    weight = [column(rw_ref[i : i + 1, :])[:, 0:1] for i in range(2)]
    mix_ref[...] = (dot(picks[0], back) * weight[0] + dot(picks[1], back) * weight[1]).astype(BF16)

    with jax.named_scope("drain"):
        wait_for(chunks(2), pass_send.at[0])

        def drain(s):
            _, used = comes(c, s)
            pl.when(goes(s))(lambda: wait_for(chunks(4), ring_send.at[s]))
            pl.when(used)(lambda: wait_for(chunks(4), pass_send.at[s]))

        loop(1, steps + 1, drain)
        for i in range(2):
            wait_for(disp.at[all_but_one], a2a_send.at[i])
        for _, sent in xs + hs:
            sent()
        o_sent()


def per_device(nz, ny, nx, *args):
    q, k, v, scale, hgain, wout, x, ngain, ids, rw, gate, up, down = args
    ta, hd2 = q.shape
    vd = v.shape[1]
    tb, dcol = x.shape
    n_ep, n_tp = 2 * nz, ny * nx
    cap = 2 * tb * ids.shape[1] // n_ep
    slots = n_ep * cap
    d, ff = gate.shape[1:]
    gate, up, down = gate.reshape(d, ff), up.reshape(d, ff), down.reshape(down.shape[1:])
    ocol = down.shape[1]
    steps = nz // 2
    vmem = pl.BlockSpec(memory_space=pltpu.VMEM)
    hbm = pl.BlockSpec(memory_space=pl.ANY)
    dma = pltpu.SemaphoreType.DMA
    return pl.pallas_call(
        functools.partial(kernel, nz, ny, nx, cap),
        out_shape=(
            jax.ShapeDtypeStruct((ta, wout.shape[1]), BF16),
            jax.ShapeDtypeStruct((tb, ocol), BF16),
        ),
        in_specs=[
            vmem, vmem, vmem, pl.BlockSpec(memory_space=pltpu.SMEM), vmem, hbm, vmem, vmem, vmem, vmem, hbm, hbm, hbm,
        ],
        out_specs=(vmem, vmem),
        scratch_shapes=[
            pltpu.VMEM((n_ep, ta, hd2), BF16),
            pltpu.VMEM((nz, vd + 16, 2 * ta), BF16),
            pltpu.VMEM((2 * hd2, 2 * ta), BF16),
            pltpu.VMEM((1, 2 * ta), F32),
            pltpu.VMEM((vd + 16, 2 * ta), F32),
            pltpu.VMEM((d // 128, 128), F32),
            pltpu.VMEM((slots, 128), F32),
            pltpu.VMEM((slots, dcol), BF16),
            pltpu.VMEM((n_tp, slots, dcol), BF16),
            pltpu.VMEM((slots, 2 * ff), F32),
            pltpu.VMEM((slots, n_tp * ff), BF16),
            pltpu.VMEM((slots, ocol), BF16),
            pltpu.VMEM((slots, ocol), BF16),
            pltpu.VMEM((ta, n_tp * vd), BF16),
            pltpu.VMEM((2, tb, slots), BF16),
            pltpu.VMEM((d, 2 * ff), BF16),
            pltpu.VMEM(down.shape, BF16),
            pltpu.VMEM(wout.shape, BF16),
            dma((4,)),
            dma((steps + 1,)),
            dma((steps + 1, 4)),
            dma((steps + 1,)),
            dma((steps + 1,)),
            dma((2,)),
            dma((3,)),
            dma((5,)),
            dma((5, 7)),
        ],
        compiler_params=pltpu.CompilerParams(
            collective_id=0, has_side_effects=True, vmem_limit_bytes=60 * 1024 * 1024
        ),
        name="layer",
    )(q, k, v, scale, hgain.reshape(1, -1), wout, x, ngain.reshape(1, -1), ids.T, rw.T, gate, up, down)


def solution(mesh):
    placed = (
        P("ep", "tp"),
        P("ep", "tp"),
        P("ep", "tp"),
        P("tp"),
        P(),
        P(None, "tp"),
        P("ep", "tp"),
        P(),
        P("ep", None),
        P("ep", None),
        P("ep", None, "tp"),
        P("ep", None, "tp"),
        P("ep", None, "tp"),
    )
    ny, nx = PLANE[mesh.shape["tp"]]
    return jax.shard_map(
        functools.partial(per_device, mesh.shape["ep"] // 2, ny, nx),
        mesh=mesh,
        in_specs=placed,
        out_specs=(P("ep", "tp"), P("ep", "tp")),
        check_vma=False,
    )
```

```python
import functools
import math

import jax
import jax.numpy as jnp
from jax import lax
from jax.experimental import pallas as pl
from jax.experimental.pallas import tpu as pltpu
from jax.sharding import PartitionSpec as P

MESH = pl.DeviceIdType.MESH
F32 = jnp.float32
BF16 = jnp.bfloat16
EPS = 1e-06
HEAD_FACTOR = 0.8
NEG = -1e30
PLANE = {16: (4, 4), 1: (1, 1)}
PLAN = (
    [("x", 0, 0), ("x", 0, 10), ("x", 1, 0)],
    {
        2: [("x", 0, 1), ("x", 0, 11)],
        3: [("x", 0, 30)],
        5: [("x", 1, 1), ("x", 0, 12), ("x", 0, 2)],
        6: [("x", 1, 11), ("x", 1, 10)],
        9: [("x", 0, 32)],
        11: [("x", 0, 33), ("x", 0, 31), ("sides", 0, 0), ("x", 1, 2), ("x", 1, 12)],
        13: [("x", 1, 30)],
        15: [("x", 0, 5)],
        17: [("x", 1, 33), ("x", 1, 31)],
        18: [("x", 1, 32), ("sides", 1, 0)],
        19: [("h", 0, 1)],
        20: [("h", 0, 11), ("h", 0, 10), ("h", 0, 12)],
        21: [("x", 1, 5)],
        22: [("h", 0, 2)],
        23: [("h", 0, 30)],
        24: [("h", 0, 31), ("h", 0, 32)],
        25: [("h", 1, 1), ("h", 1, 12), ("h", 1, 11), ("h", 1, 10)],
        26: [("h", 1, 2), ("h", 0, 33)],
        27: [("e", 0, 0)],
        28: [("h", 0, 5), ("h", 1, 30)],
        29: [("h", 1, 31), ("h", 1, 32), ("e", 0, 10)],
        30: [("h", 1, 33), ("e", 0, 1), ("e", 0, 12), ("e", 0, 11)],
        31: [("e", 0, 2), ("e", 0, 30)],
    },
    [("o", 0, 0), ("o", 0, 10), ("h", 1, 5), ("e", 0, 32), ("e", 0, 31), ("e", 0, 33), ("e", 0, 5), ("o", 0, 1), ("o", 0, 12), ("o", 0, 11), ("o", 0, 2), ("o", 0, 32), ("o", 0, 30), ("o", 0, 31), ("o", 0, 33), ("o", 0, 5)],
)


def dot(a, b):
    return lax.dot_general(a, b, (((1,), (0,)), ((), ())), preferred_element_type=F32)


def kernel(
    nz,
    ny,
    nx,
    cap,
    q_ref,
    k_ref,
    v_ref,
    scale_ref,
    hgain_ref,
    wout_hbm,
    x_ref,
    ngain_ref,
    ids_ref,
    rw_ref,
    gate_hbm,
    up_hbm,
    down_hbm,
    mixer_ref,
    mix_ref,
    kbuf,
    vbuf,
    qq,
    m_ref,
    acc,
    gs,
    ssq,
    disp,
    xbuf,
    gu,
    hbuf,
    obuf,
    rbuf,
    hobuf,
    picks,
    wgu,
    wdown,
    wout,
    w_sem,
    ring_send,
    ring_recv,
    pass_send,
    pass_recv,
    a2a_send,
    a2a_recv,
    xy_send,
    xy_recv,
):
    n_ep, n_tp = 2 * nz, ny * nx
    ta, hd2 = q_ref.shape
    vd = v_ref.shape[1]
    tb, dcol = x_ref.shape
    slots = n_ep * cap
    ff = gate_hbm.shape[1]
    ocol = wdown.shape[1]
    steps = nz // 2

    ep = lax.axis_index("ep")
    tp = lax.axis_index("tp")
    z, c = lax.div(ep, 2), lax.rem(ep, 2)
    y, x = lax.div(tp, nx), lax.rem(tp, nx)

    def at_ep(zz, cc):
        return {"ep": 2 * zz + cc}

    def remote(src, dst, ssem, rsem, dev):
        return pltpu.make_async_remote_copy(
            src_ref=src, dst_ref=dst, send_sem=ssem, recv_sem=rsem, device_id=dev, device_id_type=MESH
        )

    barrier = pltpu.get_barrier_semaphore()

    def greet_ep(i, carry):
        pl.semaphore_signal(barrier, inc=1, device_id={"ep": lax.rem(ep + i, n_ep)}, device_id_type=MESH)
        return carry

    def greet_tp(i, carry):
        pl.semaphore_signal(barrier, inc=1, device_id={"tp": lax.rem(tp + i, n_tp)}, device_id_type=MESH)
        return carry

    lax.fori_loop(1, n_ep, greet_ep, 0)
    if n_tp > 1:
        lax.fori_loop(1, n_tp, greet_tp, 0)

    w_copies = [
        pltpu.make_async_copy(gate_hbm, wgu.at[:, pl.ds(0, ff)], w_sem.at[0]),
        pltpu.make_async_copy(up_hbm, wgu.at[:, pl.ds(ff, ff)], w_sem.at[1]),
        pltpu.make_async_copy(down_hbm, wdown, w_sem.at[2]),
        pltpu.make_async_copy(wout_hbm, wout, w_sem.at[3]),
    ]
    for copy in w_copies:
        copy.start()

    v_t = v_ref[...].astype(F32).T.astype(BF16)

    @pl.when(c == 0)
    def _():
        vbuf[z, 0:vd, 0:ta] = v_t

    @pl.when(c == 1)
    def _():
        vbuf[z, 0:vd, ta : 2 * ta] = v_t

    kbuf[ep] = k_ref[...]

    def ones_rows(i, carry):
        vbuf[i, vd : vd + 16, :] = jnp.ones((16, 2 * ta), BF16)
        return carry

    lax.fori_loop(0, nz, ones_rows, 0)

    half = hd2 // 2
    q_t = (q_ref[...].astype(F32) * (math.log2(math.e) * half**-0.5)).T
    q_hi = q_t.astype(BF16)
    q_lo = (q_t - q_hi.astype(F32)).astype(BF16)
    none = jnp.zeros((half, ta), BF16)
    for i, part in enumerate((q_hi, q_lo)):
        qq[2 * half * i : 2 * half * i + half, 0:ta] = part[0:half]
        qq[2 * half * i : 2 * half * i + half, ta : 2 * ta] = none
        qq[2 * half * i + half : 2 * half * (i + 1), 0:ta] = none
        qq[2 * half * i + half : 2 * half * (i + 1), ta : 2 * ta] = part[half:]
    m_ref[...] = jnp.full(m_ref.shape, NEG, F32)
    acc[...] = jnp.zeros(acc.shape, F32)
    gu[...] = jnp.zeros(gu.shape, F32)
    ssq[...] = jnp.zeros(ssq.shape, F32)
    for i in range(gs.shape[0]):
        gs[i : i + 1, :] = ngain_ref[:, 128 * i : 128 * (i + 1)]

    def column(row):
        return jnp.broadcast_to(row, (128, tb)).T

    ids = [column(ids_ref[i : i + 1, :].astype(F32)) for i in range(2)]
    lane = lax.broadcasted_iota(jnp.int32, (tb, 128), 1).astype(F32)
    first = jnp.where(ids[0] == lane, 1.0, 0.0).astype(F32)
    second = jnp.where(ids[1] == lane, 1.0, 0.0).astype(F32)
    lower = jnp.where(
        lax.broadcasted_iota(jnp.int32, (tb, tb), 0) > lax.broadcasted_iota(jnp.int32, (tb, tb), 1), 1.0, 0.0
    ).astype(BF16)
    before_0 = dot(lower, first.astype(BF16))
    before_1 = dot(lower, second.astype(BF16)) + jnp.sum(first, axis=0, keepdims=True)
    rank_0 = jnp.sum(first * before_0, axis=1, keepdims=True)
    rank_1 = jnp.sum(second * before_1, axis=1, keepdims=True)
    slot_0 = ids[0][:, 0:1] * cap + rank_0
    slot_1 = ids[1][:, 0:1] * cap + rank_1
    slot_lane = lax.broadcasted_iota(jnp.int32, (tb, slots), 1).astype(F32)
    pick_0 = jnp.where(slot_0 == slot_lane, 1.0, 0.0).astype(F32)
    pick_1 = jnp.where(slot_1 == slot_lane, 1.0, 0.0).astype(F32)
    picks[0] = pick_0.astype(BF16)
    picks[1] = pick_1.astype(BF16)
    disp[...] = dot((pick_0 + pick_1).T.astype(BF16), x_ref[...]).astype(BF16)

    with jax.named_scope("barrier"):
        pl.semaphore_wait(barrier, (n_ep - 1) + (n_tp - 1))

    def loop(lo, hi, f):
        if not isinstance(lo, int) or not isinstance(hi, int) or hi > lo:
            lax.fori_loop(lo, hi, lambda i, carry: (f(i), carry)[1], 0)

    passes = 2

    def chip_at(k):
        away = steps - lax.div(k + 1, 2)
        return lax.rem(jnp.where(lax.rem(k, 2) == 1, z + away, z - away + nz), nz)

    def mirrored(k):
        swapped = jnp.where(lax.rem(k, 2) == 1, k + 1, k - 1)
        return jnp.where(jnp.logical_or(k == 0, k == nz - 1), k, swapped)

    def rows_of(i):
        return pl.ds(pl.multiple_of(i * cap, cap), cap)

    def dispatch_copy(i):
        k, core = lax.div(i, 2), lax.rem(i, 2)
        peer = 2 * chip_at(k) + core
        there = 2 * mirrored(k) + c
        group = lax.div(there, n_ep // passes)
        return remote(disp.at[rows_of(peer)], xbuf.at[tp, rows_of(there)], a2a_send.at[0], a2a_recv.at[group], {"ep": peer})

    def wait_for(ref, sem):
        pltpu.make_async_copy(ref, ref, sem).wait()

    def dispatched(p):
        each = n_ep // passes
        if nz == 1:
            pl.when(c != p)(lambda: wait_for(xbuf.at[0, pl.ds(0, cap)], a2a_recv.at[p]))
        else:
            wait_for(xbuf.at[0, pl.ds(0, (each - (p == passes - 1)) * cap)], a2a_recv.at[p])

    def return_copy(i):
        peer = 2 * chip_at(lax.div(i, 2)) + lax.rem(i, 2)
        return remote(obuf.at[rows_of(i)], rbuf.at[rows_of(ep)], a2a_send.at[1], a2a_recv.at[passes], {"ep": peer})

    all_but_one = pl.ds(0, (n_ep - 1) * cap)

    self_place = 2 * (nz - 1) + c

    def others(lo, hi, f):
        def each(i):
            pl.when(i != self_place)(lambda: f(i))

        loop(lo, hi, each)

    others(0, n_ep, lambda i: dispatch_copy(i).start())
    xbuf[tp, rows_of(self_place), :] = disp[rows_of(ep), :]

    def k_at(zz, cc):
        return kbuf.at[2 * zz + cc]

    def v_at(zz, cc):
        return vbuf.at[zz, pl.ds(0, vd), pl.ds(pl.multiple_of(cc * ta, 128), ta)]

    def part(owner, core, e):
        return (k_at, v_at)[e % 2](owner, core if e < 2 else 1 - core)

    next_chip = jnp.where(c == 1, lax.rem(z + 1, nz), lax.rem(z - 1 + nz, nz))

    def owner_of(core, s):
        return lax.rem(jnp.where(core == 1, z - s + nz, z + s), nz)

    def comes(core, s):
        low = nz - 2 - steps
        up, down = z - s >= 0, z + s - nz >= 0
        brought = jnp.where(core == 1, up & (s <= steps), (owner_of(core, s) <= low) & (s <= low + 1))
        return brought, brought & ((core == 1) | down)

    def goes(s):
        low = nz - 2 - steps
        return jnp.where(
            c == 1,
            (z + 1 < nz) & (z - (s - 1) >= 0) & (s <= steps),
            (owner_of(c, s - 1) <= low) & (s <= low + 1),
        )

    def hop(s, e):
        ref = part(owner_of(c, s - 1), c, e)
        return remote(ref, ref, ring_send.at[s], ring_recv.at[s, e], at_ep(next_chip, c))

    def hopped(s, e):
        ref = part(owner_of(c, s), c, e)
        return remote(ref, ref, ring_send.at[s], ring_recv.at[s, e], at_ep(next_chip, c))

    def handover(s, e):
        ref = part(owner_of(c, s), c, e)
        return remote(ref, ref, pass_send.at[s], pass_recv.at[s], at_ep(z, 1 - c))

    def chunks(n):
        return kbuf.at[pl.ds(0, min(n, n_ep))]

    for e in range(2):
        pl.when(goes(1))(lambda e=e: hop(1, e).start())
        handover(0, e).start()

    def ring_event(s, e):
        brought, used = comes(c, s)

        @pl.when(brought)
        def _():
            hopped(s, e).wait_recv()
            pl.when(goes(s + 1))(lambda: hop(s + 1, e).start())
            pl.when(used)(lambda: handover(s, e).start())

    n_tile = 256 if (2 * ta) % 256 == 0 else 2 * ta
    tiles = 2 * ta // n_tile

    def attend(owner, masked):
        keys = kbuf[pl.ds(2 * owner, 2)].reshape(2 * ta, hd2)
        keys = jnp.concatenate([keys, keys], axis=1)

        def scores(n):
            return dot(keys, qq[:, n * n_tile : (n + 1) * n_tile])

        ahead = scores(0)
        for n in range(tiles):
            s, cols = ahead, slice(n * n_tile, (n + 1) * n_tile)
            if n + 1 < tiles:
                ahead = scores(n + 1)
            if masked:
                row = lax.broadcasted_iota(jnp.int32, s.shape, 0)
                col = lax.broadcasted_iota(jnp.int32, s.shape, 1) + n * n_tile
                col = jnp.where(col >= ta, col - ta, col) + c * ta
                s = jnp.where(row <= col, s, NEG)
            old = m_ref[:, cols]
            new = jnp.maximum(old, jnp.max(s, axis=0, keepdims=True))
            weights = jnp.exp2(s - new).astype(BF16)
            shrink = jnp.exp2(old - new)
            m_ref[:, cols] = new
            acc[:, cols] = acc[:, cols] * shrink + dot(vbuf[owner], weights)

    with jax.named_scope("own_wait"):
        wait_for(chunks(2), pass_recv.at[0])
        for e in range(2, 4):
            pl.when(goes(1))(lambda e=e: hop(1, e).start())
    with jax.named_scope("own_attend"):
        attend(z, True)

    with jax.named_scope("gain"):
        w_copies[0].wait()
        w_copies[1].wait()
        w_copies[2].wait()
        gain = gs[...].T
        for i in range(gs.shape[0]):
            rows = slice(128 * i, 128 * (i + 1))
            wgu[rows, :] = (wgu[rows, :].astype(F32) * gain[:, i : i + 1]).astype(BF16)

    def plane_gather(number, rows, block, span, direct=False):
        quarter = rows // 2

        def half_stages(h):
            size_p, size_s = (nx, ny) if h == 0 else (ny, nx)
            p, s = (x, y) if h == 0 else (y, x)

            def index(ss, pp):
                ss, pp = lax.rem(ss + 4, 4), lax.rem(pp + 4, 4)
                return ss * nx + pp if h == 0 else pp * nx + ss

            rel = (0, -1, 1, 2)
            whole, low, high = (0, rows), (0, quarter), (quarter, quarter)

            def send(name, ds, dp, part):
                group = {"p": 0, "f": 1, "s": 2, "g": 6}[name[0]] + (int(name[2]) if name[0] == "s" else 0)
                ts, tp_ = {"r": (0, 1), "l": (0, -1), "o": (0, 2), "u": (1, 0), "d": (-1, 0)}[name[1]]
                ref = block(h, index(s + ds, p + dp), *part)
                remote(
                    ref, ref, xy_send.at[number], xy_recv.at[number, group], {"tp": index(s + ts, p + tp_)}
                ).start()

            def prime():
                if direct:
                    send("fo", 0, 0, whole)
                send("pr", 0, 0, whole)
                send("pl", 0, 0, whole)

            def out(j):
                send(f"su{j}", 0, rel[j], whole)
                send(f"sd{j}", 0, rel[j], whole)

            def across():
                if not direct:
                    send("fr", 0, -1, low)
                    send("fl", 0, 1, high)

            def forward(j):
                send("gu", -1, rel[j], low)
                send("gd", 1, rel[j], high)

            sends = {0: prime, 10: lambda: out(0), 1: across, 11: lambda: out(1), 12: lambda: out(2), 2: lambda: out(3)}
            for j in range(4):
                sends[30 + j] = functools.partial(forward, j)
            return sends

        if n_tp == 1:
            return lambda i: None, lambda: None
        first, second = half_stages(0), half_stages(1)
        waits = {1: (0, 4), 2: (1, 2), 30: (2, 4), 31: (3, 4), 32: (4, 4), 33: (5, 4), 5: (6, 8)}

        def both(i):
            with jax.named_scope(f"g{number}_{i}"):
                if i in waits:
                    kind, count = waits[i]
                    wait_for(span(count), xy_recv.at[number, kind])
                if i in first:
                    first[i]()
                    second[i]()

        def drained():
            wait_for(span(30), xy_send.at[number])

        return both, drained

    rows_p = slots // passes
    rows_x = rows_p // 2

    def x_block(p, h, owner, row, count):
        return xbuf.at[owner, pl.ds(p * rows_p + h * rows_x + row, count)]

    def h_block(p, h, owner, row, count):
        return hbuf.at[pl.ds(p * rows_p + h * rows_x + row, count), pl.ds(pl.multiple_of(owner * ff, 128), ff)]

    rows_a = ta // 2

    def ho_block(h, owner, row, count):
        return hobuf.at[pl.ds(h * rows_a + row, count), pl.ds(pl.multiple_of(owner * vd, 128), vd)]

    def x_span(n):
        return xbuf.at[pl.ds(0, n // 2), pl.ds(0, 2 * rows_x)]

    def h_span(n):
        return hbuf.at[pl.ds(0, 2 * rows_x), pl.ds(0, n // 2 * ff)]

    def ho_span(n):
        return hobuf.at[pl.ds(0, 2 * rows_a), pl.ds(0, n // 2 * vd)]

    xs = [plane_gather(p, rows_x, functools.partial(x_block, p), x_span) for p in range(passes)]
    hs = [plane_gather(passes + p, rows_x, functools.partial(h_block, p), h_span, True) for p in range(passes)]
    o_stage, o_sent = plane_gather(2 * passes, rows_a, ho_block, ho_span, True)

    def add_group(p, h, ds):
        at = slice(p * rows_p + h * rows_x, p * rows_p + (h + 1) * rows_x)
        if n_tp == 1:
            owners = [0]
        elif h == 0:
            owners = [lax.rem(y + ds + ny, ny) * nx + j for j in range(nx)]
        else:
            owners = [j * nx + lax.rem(x + ds + nx, nx) for j in range(ny)]
        total, squares = gu[at, :], ssq[at, :]
        for owner in owners:
            rows = xbuf[owner, at, :]
            total = total + dot(rows, wgu[pl.ds(pl.multiple_of(owner * dcol, dcol), dcol), :])
            wide = rows.astype(F32)
            wide = wide * wide
            for j in range(dcol // 128):
                squares = squares + wide[:, 128 * j : 128 * (j + 1)]
        gu[at, :] = total
        ssq[at, :] = squares

    def x_stage(p, i):
        if i == 0:
            with jax.named_scope("disp_wait"):
                dispatched(p)
        xs[p][0](i)
        with jax.named_scope("gate_up"):
            for ds in {32: (0,), 5: (2,)}.get(i, ()) if n_tp > 1 else (0,) * (i == 5):
                for h in range(2):
                    add_group(p, h, ds)
        if i == 5:
            at = slice(p * rows_p, (p + 1) * rows_p)
            mean = jnp.sum(ssq[at, :], axis=1, keepdims=True) / (n_tp * dcol)
            both = gu[at, :] * lax.rsqrt(mean + EPS)
            gate, up = both[:, 0:ff], both[:, ff : 2 * ff]
            hidden = (gate / (1.0 + jnp.exp(-gate)) * up).astype(BF16)
            hbuf[at, pl.ds(pl.multiple_of(tp * ff, 128), ff)] = hidden
            hs[p][0](0)

    def h_stage(p, i):
        hs[p][0](i)
        if i == 5:
            at = slice(p * rows_p, (p + 1) * rows_p)
            with jax.named_scope("down"):
                obuf[at, :] = dot(hbuf[at, :], wdown[...]).astype(BF16)
            others(2 * nz // passes * p, 2 * nz // passes * (p + 1), lambda j: return_copy(j).start())
            if p == passes - 1:
                rbuf[rows_of(ep), :] = obuf[rows_of(self_place), :]

    def heads(i):
        if i == 0:
            maps = acc[0:vd, :] / acc[vd : vd + 1, :]
            mixed = maps[:, 0:ta] - scale_ref[0] * maps[:, ta : 2 * ta]
            mean_sq = jnp.mean(mixed * mixed, axis=0, keepdims=True)
            head = (mixed * lax.rsqrt(mean_sq + EPS)).T * hgain_ref[...] * HEAD_FACTOR
            hobuf[:, pl.ds(pl.multiple_of(tp * vd, 128), vd)] = head.astype(BF16)
        o_stage(i)

    early = nz // 4

    def run(items):
        for what, p, i in items:
            if what == "sides":
                if n_tp > 1:
                    with jax.named_scope("gate_up"):
                        for ds in (-1, 1):
                            for h in range(2):
                                add_group(p, h, ds)
            elif what == "e":
                pl.when(z < early)(functools.partial(heads, i))
            elif what == "o":
                pl.when(z >= early)(functools.partial(heads, i))
            else:
                (x_stage if what == "x" else h_stage)(p, i)

    def use(core, s):
        _, used = comes(core, s)

        @pl.when(used & (s >= 1))
        def _():
            @pl.when(c != core)
            def _():
                with jax.named_scope("handed"):
                    wait_for(chunks(4), pass_recv.at[s])

            with jax.named_scope("attend"):
                attend(owner_of(core, s), False)

    run(PLAN[0])

    def tick(s):
        for e in range(4):
            with jax.named_scope("ring"):
                ring_event(s, e)
            for at, items in PLAN[1].items():
                if at % 4 == e and at // 4 + 1 <= steps + 1:
                    pl.when(s == at // 4 + 1)(functools.partial(run, items))
            if e % 2 == 0:
                use(e // 2, s - 1)

    loop(1, steps + 2, tick)
    for at, items in PLAN[1].items():
        if at // 4 + 1 > steps + 1:
            run(items)
    run(PLAN[2])

    w_copies[3].wait()
    with jax.named_scope("outproj"):
        mixer_ref[...] = dot(hobuf[...], wout[...]).astype(BF16)

    with jax.named_scope("ret_wait"):
        wait_for(rbuf.at[all_but_one], a2a_recv.at[passes])
    back = rbuf[...]
    weight = [column(rw_ref[i : i + 1, :])[:, 0:1] for i in range(2)]
    mix_ref[...] = (dot(picks[0], back) * weight[0] + dot(picks[1], back) * weight[1]).astype(BF16)

    with jax.named_scope("drain"):
        wait_for(chunks(2), pass_send.at[0])

        def drain(s):
            _, used = comes(c, s)
            pl.when(goes(s))(lambda: wait_for(chunks(4), ring_send.at[s]))
            pl.when(used)(lambda: wait_for(chunks(4), pass_send.at[s]))

        loop(1, steps + 1, drain)
        for i in range(2):
            wait_for(disp.at[all_but_one], a2a_send.at[i])
        for _, sent in xs + hs:
            sent()
        o_sent()


def per_device(nz, ny, nx, *args):
    q, k, v, scale, hgain, wout, x, ngain, ids, rw, gate, up, down = args
    ta, hd2 = q.shape
    vd = v.shape[1]
    tb, dcol = x.shape
    n_ep, n_tp = 2 * nz, ny * nx
    cap = 2 * tb * ids.shape[1] // n_ep
    slots = n_ep * cap
    d, ff = gate.shape[1:]
    gate, up, down = gate.reshape(d, ff), up.reshape(d, ff), down.reshape(down.shape[1:])
    ocol = down.shape[1]
    steps = nz // 2
    vmem = pl.BlockSpec(memory_space=pltpu.VMEM)
    hbm = pl.BlockSpec(memory_space=pl.ANY)
    dma = pltpu.SemaphoreType.DMA
    return pl.pallas_call(
        functools.partial(kernel, nz, ny, nx, cap),
        out_shape=(
            jax.ShapeDtypeStruct((ta, wout.shape[1]), BF16),
            jax.ShapeDtypeStruct((tb, ocol), BF16),
        ),
        in_specs=[
            vmem, vmem, vmem, pl.BlockSpec(memory_space=pltpu.SMEM), vmem, hbm, vmem, vmem, vmem, vmem, hbm, hbm, hbm,
        ],
        out_specs=(vmem, vmem),
        scratch_shapes=[
            pltpu.VMEM((n_ep, ta, hd2), BF16),
            pltpu.VMEM((nz, vd + 16, 2 * ta), BF16),
            pltpu.VMEM((2 * hd2, 2 * ta), BF16),
            pltpu.VMEM((1, 2 * ta), F32),
            pltpu.VMEM((vd + 16, 2 * ta), F32),
            pltpu.VMEM((d // 128, 128), F32),
            pltpu.VMEM((slots, 128), F32),
            pltpu.VMEM((slots, dcol), BF16),
            pltpu.VMEM((n_tp, slots, dcol), BF16),
            pltpu.VMEM((slots, 2 * ff), F32),
            pltpu.VMEM((slots, n_tp * ff), BF16),
            pltpu.VMEM((slots, ocol), BF16),
            pltpu.VMEM((slots, ocol), BF16),
            pltpu.VMEM((ta, n_tp * vd), BF16),
            pltpu.VMEM((2, tb, slots), BF16),
            pltpu.VMEM((d, 2 * ff), BF16),
            pltpu.VMEM(down.shape, BF16),
            pltpu.VMEM(wout.shape, BF16),
            dma((4,)),
            dma((steps + 1,)),
            dma((steps + 1, 4)),
            dma((steps + 1,)),
            dma((steps + 1,)),
            dma((2,)),
            dma((3,)),
            dma((5,)),
            dma((5, 7)),
        ],
        compiler_params=pltpu.CompilerParams(
            collective_id=0, has_side_effects=True, vmem_limit_bytes=60 * 1024 * 1024
        ),
        name="layer",
    )(q, k, v, scale, hgain.reshape(1, -1), wout, x, ngain.reshape(1, -1), ids.T, rw.T, gate, up, down)


def solution(mesh):
    placed = (
        P("ep", "tp"),
        P("ep", "tp"),
        P("ep", "tp"),
        P("tp"),
        P(),
        P(None, "tp"),
        P("ep", "tp"),
        P(),
        P("ep", None),
        P("ep", None),
        P("ep", None, "tp"),
        P("ep", None, "tp"),
        P("ep", None, "tp"),
    )
    ny, nx = PLANE[mesh.shape["tp"]]
    return jax.shard_map(
        functools.partial(per_device, mesh.shape["ep"] // 2, ny, nx),
        mesh=mesh,
        in_specs=placed,
        out_specs=(P("ep", "tp"), P("ep", "tp")),
        check_vma=False,
    )
```
